32 devices in a mesh: ep: 8 (over z, x), tp: 4 (over y, core).
Axes of the slice: x: 2, y: 2, z: 4, core: 2. Of those that a mesh axis runs over, the one named last changes fastest.
Arguments:
- stream: bfloat16 [2048, 3072], P('ep'), may hold values from -30 to 30
- ffn_gain: bfloat16 [3072], replicated, may hold values from 0.099609375 to 1.8984375
- chosen: int32 [8, 256], replicated, may hold values from 0 to 2047, as said below
- affinity: float32 [8, 256], P('ep'), may hold values from 0.5 to 2
- w_gate: bfloat16 [8, 3072, 3072], P('ep', None, 'tp'), may hold values from -0.109375 to 0.109375
- w_up: bfloat16 [8, 3072, 3072], P('ep', None, 'tp'), may hold values from -0.109375 to 0.109375
- w_down: bfloat16 [8, 3072, 3072], P('ep', 'tp'), may hold values from -0.109375 to 0.109375
- final_gain: bfloat16 [3072], P('tp'), may hold values from 0.099609375 to 1.8984375
Outputs:
- normed: bfloat16 [2048, 3072], P('ep', 'tp')
The draws below stay inside these ranges and needn't reach their ends.
Inputs may be any that keep to these rules, and one draw needn't show every extreme that they name: `chosen`: row e holds 256 distinct token numbers in ascending order. Of the 256 tokens of one index of ep, each expert reads at least one and at most 48; in every draw some expert reads exactly 48 from some index.
All inputs are finite; a program needn't handle non-finite values.
Results may differ from the reference program's by a relative error of at most 0.015.
Values may be sent and summed in bfloat16 or wider, within the bound.
A program may use at most 128 MiB of HBM per device.

```python
import math
import jax
import jax.numpy as jnp
from jax import lax

D = 3072
FF = 3072
TOK_DEV = 256
TOKENS = 2048
EXPERTS = 8
CAP = 256
N_EP = 8
N_TP = 4


def draw_stream(key, part):
    key_base, key_rows, key_cols = jax.random.split(key, 3)
    ramp = jnp.arange(D, dtype=jnp.float32) / D
    columns = jnp.exp(math.log(0.6) + ramp * math.log(3.0)) * jnp.exp(jax.random.uniform(key_cols, (D,), jnp.float32, -0.3, 0.3))
    base = jnp.clip(jax.random.normal(key_base, (TOKENS, D), jnp.float32), -4.0, 4.0)
    rows_scale = jnp.exp(jax.random.uniform(key_rows, (TOKENS, 1), jnp.float32, math.log(0.3), math.log(3.0)))
    return (base * rows_scale * columns[None, :]).astype(jnp.bfloat16)


def draw_chosen(key, part):
    mean_count = TOK_DEV // 8
    spread = TOK_DEV // 16
    pairs = N_EP // 2
    key_diff, key_pick, key_sign, key_score = jax.random.split(key, 4)
    diff = jax.random.randint(key_diff, (EXPERTS, pairs), -spread, spread + 1)
    forced = jax.random.randint(key_pick, (EXPERTS,), 0, pairs)
    signs = jax.random.randint(key_sign, (EXPERTS,), 0, 2) * 2 - 1
    diff = jnp.where(jnp.arange(pairs)[None, :] == forced[:, None], signs[:, None] * spread, diff)
    counts = jnp.stack([mean_count + diff, mean_count - diff], axis=2).reshape(EXPERTS, N_EP)
    scores = jax.random.randint(key_score, (EXPERTS, N_EP, TOK_DEV), 0, 65536) * TOK_DEV + jnp.arange(TOK_DEV)[None, None, :]
    ranks = jnp.argsort(jnp.argsort(scores, axis=-1), axis=-1)
    selected = (ranks < counts[:, :, None]).reshape(EXPERTS, TOKENS)
    positions = jnp.arange(TOKENS, dtype=jnp.int32)[None, :]
    keyed = jnp.where(selected, positions, positions + TOKENS)
    return jnp.sort(keyed, axis=-1)[:, :CAP].astype(jnp.int32)


def block_scale(own_key, shape, cuts, smallest, high):
    gain = 1.0
    for position, shards_of in cuts:
        steps = jax.random.uniform(jax.random.fold_in(jax.random.fold_in(own_key, 6), position), (shards_of,), jnp.float32, smallest / len(cuts), high / len(cuts))
        gain = gain * jnp.repeat(jnp.exp(steps), shape[position] // shards_of).reshape((-1,) + (1,) * (len(shape) - 1 - position))
    return gain


def centred(own_key, dims, scale, bound, shards=(), kind=jnp.bfloat16):
    values = jax.random.normal(own_key, dims, jnp.float32) * scale
    if len(shards) > 0:
        values = block_scale(own_key, dims, shards, -0.22, 0.18) * values
    return jnp.clip(values, min=-bound, max=bound).astype(kind)


def setup_inputs(seed: int = 0) -> dict:
    key_of = jax.random.split(jax.random.key(seed), 9)
    stream = draw_stream(jax.random.fold_in(key_of[8], 71), 0)
    ffn_gain = jnp.clip(1.0 + 0.18 * jax.random.normal(key_of[1], (D,), jnp.float32), 0.099609375, 1.8984375).astype(jnp.bfloat16)
    chosen = draw_chosen(jax.random.fold_in(key_of[8], 71), 0)
    affinity = jnp.clip(jnp.exp(math.log(2.0) - 1.3862944 * jax.random.uniform(key_of[3], (EXPERTS, CAP), jnp.float32) ** block_scale(key_of[3], (EXPERTS, CAP), ((0, 8),), -0.2, 0.2)), 0.5, 2.0)
    w_gate = centred(key_of[4], (EXPERTS, D, FF), D ** -0.5, 0.109375, ((0, 8), (2, 4)))
    w_up = centred(key_of[5], (EXPERTS, D, FF), D ** -0.5, 0.109375, ((0, 8), (2, 4)))
    w_down = centred(key_of[6], (EXPERTS, FF, D), FF ** -0.5, 0.109375, ((0, 8), (1, 4)))
    final_gain = jnp.clip(1.0 + 0.18 * jax.random.normal(key_of[7], (D,), jnp.float32), 0.099609375, 1.8984375).astype(jnp.bfloat16)
    return dict(stream=stream, ffn_gain=ffn_gain, chosen=chosen, affinity=affinity, w_gate=w_gate, w_up=w_up, w_down=w_down, final_gain=final_gain)


EPSILON = 1e-06

def reference(stream, ffn_gain, chosen, affinity, w_gate, w_up, w_down, final_gain):
    widened = stream.astype(jnp.float32)
    scale_in = lax.rsqrt(lax.optimization_barrier(jnp.mean(widened * widened, axis=-1, keepdims=True)) + EPSILON)
    normed_in = (widened * scale_in * ffn_gain.astype(jnp.float32)).astype(jnp.bfloat16)
    block = FF // N_TP

    def one_expert(update, items):
        token_ids, weights, gate_rows, up_rows, down_rows = items
        picked = normed_in[token_ids]
        gate = jnp.dot(picked, gate_rows, preferred_element_type=jnp.float32)
        up = jnp.dot(picked, up_rows, preferred_element_type=jnp.float32)
        hidden = (jax.nn.silu(gate) * up).astype(jnp.bfloat16)
        blocks = hidden.reshape(CAP, N_TP, block).astype(jnp.float32)
        down_blocks = down_rows.reshape(N_TP, block, D).astype(jnp.float32)
        partial_value = jnp.einsum('cjf,jfd->jcd', blocks, down_blocks).astype(jnp.bfloat16)
        summed = lax.optimization_barrier(jnp.sum(partial_value.astype(jnp.float32), axis=0))
        result = (summed * weights[:, None]).astype(jnp.bfloat16)
        return (update.at[token_ids].add(result.astype(jnp.float32)), None)
    update, unused = lax.scan(one_expert, jnp.zeros((TOKENS, D), jnp.float32), (chosen, affinity, w_gate, w_up, w_down))
    merged = widened + update
    scale_out = lax.rsqrt(lax.optimization_barrier(jnp.mean(merged * merged, axis=-1, keepdims=True)) + EPSILON)
    return (merged * scale_out * final_gain.astype(jnp.float32)).astype(jnp.bfloat16)
```

```python
import functools

import jax
import jax.numpy as jnp
from jax import lax
from jax.experimental import pallas as pl
from jax.experimental.pallas import tpu as pltpu
from jax.sharding import PartitionSpec as P

EPSILON = 1e-06
F32 = jnp.float32
BF16 = jnp.bfloat16
I32 = jnp.int32
MESH = pl.DeviceIdType.MESH


def layer(
    experts, tp, groups, fold, slots,
    stream_hbm, gain_hbm, chosen_hbm, aff_hbm, wg_hbm, wu_hbm, wd_hbm, fgain_hbm,
    out_ref,
    x_v, xn_v, gain_v, gainf_v, chosen_v, aff_v, fgain_v, wg_v, wu_v, wd_v,
    sel_v, place_v, pack_v, spread_v, affc_v,
    send_v, recv_v, piece_v, accg_v, accu_v, hidden_v,
    psend_v, pown_v, prec_v, ysend_v, yrec_v, leave_v, ret_v, merged_v, ssq_v,
    x_sem, s_sem, wg_sem, wu_sem, wd_sem,
    dsend, drecv, gsend, grecv, fsend, frecv, psend, precv, ysend, yrecv,
    rsend, rrecv, qsend, qrecv,
):
    me = lax.axis_index("ep")
    col = lax.axis_index("tp")
    tok, width = x_v.shape
    share = width // tp
    fw = share // fold
    caps = chosen_v.shape[1]
    cg = caps // groups
    sg = slots // groups
    mr = sg * fold
    rows = experts * mr
    chips = tp // 2
    y = col // 2
    core = col % 2
    partner = y * 2 + 1 - core

    barrier = pltpu.get_barrier_semaphore()
    for r in range(1, experts):
        pl.semaphore_signal(barrier, inc=1, device_id={"ep": (me + r) % experts}, device_id_type=MESH)
    for r in range(1, tp):
        pl.semaphore_signal(barrier, inc=1, device_id={"tp": (col + r) % tp}, device_id_type=MESH)

    small = []
    for n, (src, dst) in enumerate(
        ((chosen_hbm, chosen_v), (gain_hbm, gain_v), (aff_hbm, aff_v), (fgain_hbm, fgain_v))
    ):
        copy = pltpu.make_async_copy(src, dst, s_sem.at[n])
        copy.start()
        small.append(copy)
    pieces = x_sem.shape[0]
    xrows = tok // pieces
    x_copies = []
    for i in range(pieces):
        at = pl.ds(i * xrows, xrows)
        copy = pltpu.make_async_copy(stream_hbm.at[at, :], x_v.at[at, :], x_sem.at[i])
        copy.start()
        x_copies.append(copy)

    small[0].wait()
    base = (me * tok).astype(F32)
    lane_cap = lax.broadcasted_iota(I32, (mr, caps), 1)
    lane_tok = lax.broadcasted_iota(I32, (mr, tok), 1).astype(F32)
    sub = lax.broadcasted_iota(I32, (mr, 1), 0)
    sub_half = sum((jnp.where(sub >= h * sg, 1, 0) for h in range(1, fold)), jnp.zeros((mr, 1), I32))
    sub_slot = sub - sg * sub_half

    def build_sel(e, carry):
        row = chosen_v[pl.ds(e, 1), :].astype(F32)
        start = jnp.sum(jnp.where(row < base, 1.0, 0.0), axis=1, keepdims=True).astype(I32)
        for g in range(groups):
            first = start + ((g - start) & (groups - 1))
            hit = lane_cap == first + groups * sub_slot
            token = jnp.sum(jnp.where(hit, row + 1.0, 0.0), axis=1, keepdims=True) - 1.0 - base
            for h in range(fold):
                one = (token == lane_tok) & (sub_half == h)
                sel_v[g, e, :, h * tok:(h + 1) * tok] = jnp.where(one, 1.0, 0.0).astype(BF16)
        return carry

    lax.fori_loop(0, experts, build_sel, 0, unroll=experts <= 8)

    small[1].wait()
    gainf_v[...] = gain_v[...].astype(F32)
    lines = share // 128
    gain = jnp.concatenate(
        [gainf_v[pl.ds(col * lines + i, 1), :] for i in range(lines)], axis=1
    )
    step = 32
    for i in range(pieces):
        x_copies[i].wait()
        if i == pieces - 1:
            w_copies = {}
            for r in range(chips):
                for c in range(2):
                    s = r * 2 + c
                    other = core if c == 0 else 1 - core
                    frm = ((y + chips - r) % chips) * 2 + other
                    for n, (src, dst, sem) in enumerate(((wg_hbm, wg_v, wg_sem), (wu_hbm, wu_v, wu_sem))):
                        copy = pltpu.make_async_copy(
                            src.at[pl.ds(frm * share, share), :],
                            dst.at[pl.ds(s * share, share), :],
                            sem.at[s],
                        )
                        copy.start()
                        w_copies[n, s] = copy
            for r in list(range(1, chips)) + [0]:
                for c in (1, 0):
                    s = r * 2 + c
                    other = core if c == 0 else 1 - core
                    to = ((y + r) % chips) * 2 + other
                    copy = pltpu.make_async_copy(
                        wd_hbm.at[:, pl.ds(pl.multiple_of(to * share, 128), share)],
                        wd_v.at[s], wd_sem.at[s],
                    )
                    copy.start()
                    w_copies[2, s] = copy
        for b in range(xrows // step):
            at = pl.ds(i * xrows + b * step, step)
            block = x_v[at, :].astype(F32)
            scale = lax.rsqrt(jnp.sum(block * block, axis=1, keepdims=True) / width + EPSILON)
            own = x_v[at, pl.ds(pl.multiple_of(col * share, 128), share)].astype(F32)
            normed = (own * scale * gain).astype(BF16)
            for h in range(fold):
                xn_v[pl.ds(h * tok + i * xrows + b * step, step), :] = normed[:, h * fw:(h + 1) * fw]

    finish = []
    far_first = sorted(range(1, experts), key=lambda r: -min(r, experts - r))

    def exchange(g, src, dst, ssem, rsem):
        for r in far_first:
            to = (me + r) % experts
            copy = pltpu.make_async_remote_copy(
                src_ref=src.at[g, to], dst_ref=dst.at[g, me],
                send_sem=ssem.at[g], recv_sem=rsem.at[g],
                device_id={"ep": to}, device_id_type=MESH,
            )
            copy.start()
        dst[g, me] = src[g, me]
        finish.append(whole_exchange(g, src, dst, ssem, rsem))

    def whole_exchange(g, src, dst, ssem, rsem):
        others = pl.ds(0, experts - 1)
        return pltpu.make_async_remote_copy(
            src_ref=src.at[g, others], dst_ref=dst.at[g, others],
            send_sem=ssem.at[g], recv_sem=rsem.at[g],
            device_id={"ep": (me + 1) % experts}, device_id_type=MESH,
        )

    def exchange_wait(g, src, dst, ssem, rsem):
        whole_exchange(g, src, dst, ssem, rsem).wait_recv()

    for g in range(groups):
        out = jnp.dot(sel_v[g].reshape(rows, fold * tok), xn_v[...], preferred_element_type=F32)
        send_v[g] = out.astype(BF16).reshape(experts, mr, fw)
        if g == 0:
            pl.semaphore_wait(barrier, experts - 1 + tp - 1)
        exchange(g, send_v, recv_v, dsend, drecv)

    own_row = chosen_v[pl.ds(me, 1), :].astype(F32)

    def positions(axis):
        shape = (rows, 1) if axis == 0 else (1, rows)
        j = lax.broadcasted_iota(I32, shape, axis)
        start = jnp.zeros(shape, F32)
        end = jnp.zeros(shape, F32)
        within = j
        cut = jnp.zeros((1, 1), F32)
        for d in range(experts):
            mine = (j >= d * mr) & (j < (d + 1) * mr)
            after = jnp.sum(jnp.where(own_row < float((d + 1) * tok), 1.0, 0.0), axis=1, keepdims=True)
            start = start + jnp.where(mine, cut, 0.0)
            end = end + jnp.where(mine, after, 0.0)
            within = within - jnp.where(mine, d * mr, 0)
            cut = after
        half = sum((jnp.where(within >= h * sg, 1, 0) for h in range(1, fold)), jnp.zeros(shape, I32))
        return start.astype(I32), end.astype(I32), half, within - sg * half

    for axis, dst in ((1, pack_v), (0, spread_v)):
        start, end, half, slot = positions(axis)
        for g in range(groups):
            want = start + ((g - start) & (groups - 1)) + groups * slot
            want = jnp.where(want < end, want, -1)
            for h in range(fold):
                aim = jnp.where(half == h, want, -1)
                if axis == 1:
                    pick = lax.broadcasted_iota(I32, (cg, rows), 0) * groups + g
                    pack_v[g, h * cg:(h + 1) * cg, :] = jnp.where(pick == aim, 1.0, 0.0).astype(BF16)
                else:
                    pick = lax.broadcasted_iota(I32, (rows, cg), 1) * groups + g
                    spread_v[g, :, h * cg:(h + 1) * cg] = jnp.where(pick == aim, 1.0, 0.0).astype(BF16)

    small[2].wait()
    for g in range(groups):
        lane = lax.broadcasted_iota(I32, (cg, caps), 1)
        pick = lax.broadcasted_iota(I32, (cg, caps), 0) * groups + g
        affc_v[g] = jnp.sum(jnp.where(lane == pick, aff_v[...], 0.0), axis=1, keepdims=True)

    for g in range(groups):
        whole = sel_v[g].reshape(rows, fold * tok).astype(F32)
        place_v[g] = whole.T.astype(BF16)

    def gather_start(g):
        exchange_wait(g, send_v, recv_v, dsend, drecv)
        got = recv_v[g].reshape(rows, fw)
        piece_v[g, 0] = jnp.dot(pack_v[g], got, preferred_element_type=F32).astype(BF16)
        for r in range(1, chips):
            to = ((y + r) % chips) * 2 + core
            copy = pltpu.make_async_remote_copy(
                src_ref=piece_v.at[g, 0], dst_ref=piece_v.at[g, 2 * r],
                send_sem=gsend.at[g, r], recv_sem=grecv.at[g, r],
                device_id={"tp": to}, device_id_type=MESH,
            )
            copy.start()
            finish.append(copy)
        forward(g, 0)

    def forward_copy(g, r):
        return pltpu.make_async_remote_copy(
            src_ref=piece_v.at[g, 2 * r], dst_ref=piece_v.at[g, 2 * r + 1],
            send_sem=fsend.at[g, r], recv_sem=frecv.at[g, r],
            device_id={"tp": partner}, device_id_type=MESH,
        )

    def forward(g, r):
        copy = forward_copy(g, r)
        copy.start()
        finish.append(copy)

    def gather_forward(g):
        for r in range(1, chips):
            frm = ((y + chips - r) % chips) * 2 + core
            pltpu.make_async_remote_copy(
                src_ref=piece_v.at[g, 0], dst_ref=piece_v.at[g, 2 * r],
                send_sem=gsend.at[g, r], recv_sem=grecv.at[g, r],
                device_id={"tp": frm}, device_id_type=MESH,
            ).wait_recv()
            forward(g, r)

    waited = set()

    def weight_wait(n, s):
        if (n, s) not in waited:
            waited.add((n, s))
            w_copies[n, s].wait()

    def contract(g, lo, hi):
        taken = jnp.concatenate(
            [piece_v[g, s, h * cg:(h + 1) * cg, :] for s in range(lo, hi) for h in range(fold)], axis=1
        )
        for n in range(2):
            for s in range(lo, hi):
                weight_wait(n, s)
        at = pl.ds(lo * share, (hi - lo) * share)
        gate = jnp.dot(taken, wg_v[at, :], preferred_element_type=F32)
        up = jnp.dot(taken, wu_v[at, :], preferred_element_type=F32)
        return gate, up

    def near(g):
        forward_copy(g, 0).wait_recv()
        gate, up = contract(g, 0, 2)
        accg_v[g] = gate
        accu_v[g] = up

    def pair_copy(g, r):
        return pltpu.make_async_remote_copy(
            src_ref=psend_v.at[g, r], dst_ref=prec_v.at[g, r],
            send_sem=psend.at[g, r], recv_sem=precv.at[g, r],
            device_id={"tp": partner}, device_id_type=MESH,
        )

    def far(g):
        for r in range(1, chips):
            forward_copy(g, r).wait_recv()
        gate, up = contract(g, 2, tp)
        gate = gate + accg_v[g]
        up = up + accu_v[g]
        hidden_v[g] = (gate / (1.0 + jnp.exp(-gate)) * up).astype(BF16)
        for turns in (list(range(1, chips)), [0]):
            for r in turns:
                weight_wait(2, 2 * r + 1)
                psend_v[g, r] = jnp.dot(hidden_v[g], wd_v[2 * r + 1], preferred_element_type=F32).astype(BF16)
                copy = pair_copy(g, r)
                copy.start()
                finish.append(copy)
            for r in turns:
                weight_wait(2, 2 * r)
                pown_v[g, r] = jnp.dot(hidden_v[g], wd_v[2 * r], preferred_element_type=F32)

    def chip_copy(g, r):
        to = ((y + r) % chips) * 2 + core
        return pltpu.make_async_remote_copy(
            src_ref=ysend_v.at[g, r], dst_ref=yrec_v.at[g, r],
            send_sem=ysend.at[g, r], recv_sem=yrecv.at[g, r],
            device_id={"tp": to}, device_id_type=MESH,
        )

    def cross(g):
        for r in range(1, chips):
            pair_copy(g, r).wait_recv()
            ysend_v[g, r] = (pown_v[g, r] + prec_v[g, r].astype(F32)).astype(BF16)
            copy = chip_copy(g, r)
            copy.start()
            finish.append(copy)

    def leave(g):
        pair_copy(g, 0).wait_recv()
        total = pown_v[g, 0] + prec_v[g, 0].astype(F32)
        for r in range(1, chips):
            chip_copy(g, r).wait_recv()
            total = total + yrec_v[g, r].astype(F32)
        weighted = (total * affc_v[g]).astype(BF16)
        folded = jnp.concatenate([weighted[:, h * fw:(h + 1) * fw] for h in range(fold)], axis=0)
        out = jnp.dot(spread_v[g], folded, preferred_element_type=F32)
        leave_v[g] = out.astype(BF16).reshape(experts, mr, fw)
        exchange(g, leave_v, ret_v, rsend, rrecv)

    def settle(g):
        exchange_wait(g, leave_v, ret_v, rsend, rrecv)
        update = jnp.dot(place_v[g], ret_v[g].reshape(rows, fw), preferred_element_type=F32)
        if g == 0:
            for h in range(fold):
                at = pl.ds(pl.multiple_of(col * share + h * fw, 128), fw)
                merged_v[h * tok:(h + 1) * tok, :] = x_v[:, at].astype(F32) + update[h * tok:(h + 1) * tok, :]
        else:
            merged_v[...] = merged_v[...] + update

    stages = {
        "s1": gather_start, "s2": gather_forward, "a": near, "b": far, "x": cross, "l": leave, "r": settle,
    }
    if groups == 4:
        order = ORDER4
    else:
        order = [f"{name}.{g}" for name in ("s1", "s2", "a", "b", "x", "l", "r") for g in range(groups)]
    for item in order:
        name, g = item.split(".")
        with jax.named_scope(name + g):
            stages[name](int(g))

    square = 128
    eye = (
        lax.broadcasted_iota(I32, (square, square), 0)
        == lax.broadcasted_iota(I32, (square, square), 1)
    )
    merged = merged_v[...]
    both = jnp.sum(merged * merged, axis=1, keepdims=True)
    squares = both[0:tok]
    for h in range(1, fold):
        squares = squares + both[h * tok:(h + 1) * tok]
    for b in range(tok // square):
        line = jnp.sum(
            jnp.where(eye, squares[b * square:(b + 1) * square, :], 0.0), axis=0, keepdims=True
        )
        ssq_v[0, :, b * square:(b + 1) * square] = jnp.broadcast_to(line, (8, square))

    def square_copy(r):
        return pltpu.make_async_remote_copy(
            src_ref=ssq_v.at[0], dst_ref=ssq_v.at[r],
            send_sem=qsend.at[r], recv_sem=qrecv.at[r],
            device_id={"tp": (col + r) % tp}, device_id_type=MESH,
        )

    for r in range(1, tp):
        copy = square_copy(r)
        copy.start()
        finish.append(copy)
    small[3].wait()
    closing = fgain_v[...].astype(F32)
    fgain = jnp.concatenate([closing[i:i + 1, :] for i in range(lines)], axis=1)
    sums = ssq_v[0]
    with jax.named_scope("sqw"):
        for r in range(1, tp):
            square_copy(r).wait_recv()
            sums = sums + ssq_v[r]
    scales = lax.rsqrt(sums[0:1, :] / width + EPSILON)
    for b in range(tok // square):
        line = scales[:, b * square:(b + 1) * square]
        column = jnp.sum(jnp.where(eye, line, 0.0), axis=1, keepdims=True)
        for h in range(fold):
            part = merged_v[h * tok + b * square:h * tok + (b + 1) * square, :]
            out_ref[b * square:(b + 1) * square, h * fw:(h + 1) * fw] = (
                part * column * fgain[:, h * fw:(h + 1) * fw]
            ).astype(BF16)

    with jax.named_scope("fin"):
        for copy in finish:
            copy.wait_send()


ORDER4 = [
    "s1.0", "a.0", "s1.1", "s2.0", "b.0", "s1.2", "a.1", "s2.1", "x.0", "a.2", "b.1",
    "s1.3", "s2.2", "x.1", "l.0", "b.2", "a.3", "s2.3", "x.2", "l.1", "b.3", "x.3", "l.2",
    "r.0", "l.3", "r.1", "r.2", "r.3",
]


def on_device(stream, ffn_gain, chosen, affinity, w_gate, w_up, w_down, final_gain):
    tok, width = stream.shape
    experts, caps = chosen.shape
    tp = lax.axis_size("tp")
    share = width // tp
    hid = w_gate.shape[2]
    slots = 3 * tok // 16
    groups, fold = (4, 2) if share % 256 == 0 else (2, 1)
    fw = share // fold
    cg = caps // groups
    mr = slots // groups * fold
    rows = experts * mr
    chips = tp // 2
    hbm = pl.BlockSpec(memory_space=pltpu.HBM)
    dma = pltpu.SemaphoreType.DMA
    buffers = [
        pltpu.VMEM((tok, width), BF16),
        pltpu.VMEM((fold * tok, fw), BF16),
        pltpu.VMEM((width // 128, 128), BF16),
        pltpu.VMEM((width // 128, 128), F32),
        pltpu.VMEM((experts, caps), I32),
        pltpu.VMEM((1, caps), F32),
        pltpu.VMEM((share // 128, 128), BF16),
        pltpu.VMEM((width, hid), BF16),
        pltpu.VMEM((width, hid), BF16),
        pltpu.VMEM((tp, hid, share), BF16),
        pltpu.VMEM((groups, experts, mr, fold * tok), BF16),
        pltpu.VMEM((groups, fold * tok, rows), BF16),
        pltpu.VMEM((groups, fold * cg, rows), BF16),
        pltpu.VMEM((groups, rows, fold * cg), BF16),
        pltpu.VMEM((groups, cg, 1), F32),
        pltpu.VMEM((groups, experts, mr, fw), BF16),
        pltpu.VMEM((groups, experts, mr, fw), BF16),
        pltpu.VMEM((groups, tp, fold * cg, fw), BF16),
        pltpu.VMEM((groups, cg, hid), F32),
        pltpu.VMEM((groups, cg, hid), F32),
        pltpu.VMEM((groups, cg, hid), BF16),
        pltpu.VMEM((groups, chips, cg, share), BF16),
        pltpu.VMEM((groups, chips, cg, share), F32),
        pltpu.VMEM((groups, chips, cg, share), BF16),
        pltpu.VMEM((groups, chips, cg, share), BF16),
        pltpu.VMEM((groups, chips, cg, share), BF16),
        pltpu.VMEM((groups, experts, mr, fw), BF16),
        pltpu.VMEM((groups, experts, mr, fw), BF16),
        pltpu.VMEM((fold * tok, fw), F32),
        pltpu.VMEM((tp, 8, tok), F32),
    ]
    return pl.pallas_call(
        functools.partial(layer, experts, tp, groups, fold, slots),
        out_shape=pltpu.VMEM((tok, share), BF16),
        in_specs=[hbm] * 8,
        out_specs=pl.BlockSpec(memory_space=pltpu.VMEM),
        scratch_shapes=buffers + [
            dma((4,)), dma((4,)), dma((tp,)), dma((tp,)), dma((tp,)),
            dma((groups,)), dma((groups,)),
            dma((groups, chips)), dma((groups, chips)),
            dma((groups, chips)), dma((groups, chips)),
            dma((groups, chips)), dma((groups, chips)),
            dma((groups, chips)), dma((groups, chips)),
            dma((groups,)), dma((groups,)),
            dma((tp,)), dma((tp,)),
        ],
        compiler_params=pltpu.CompilerParams(
            collective_id=0, has_side_effects=True, vmem_limit_bytes=56 * 1024 * 1024
        ),
        name="layer",
    )(
        stream,
        ffn_gain.reshape(width // 128, 128),
        chosen,
        affinity,
        w_gate[0],
        w_up[0],
        w_down[0],
        final_gain.reshape(share // 128, 128),
    )


def solution(mesh):
    return jax.shard_map(
        on_device,
        mesh=mesh,
        in_specs=(
            P("ep", None),
            P(),
            P(),
            P("ep", None),
            P("ep", None, "tp"),
            P("ep", None, "tp"),
            P("ep", "tp", None),
            P("tp"),
        ),
        out_specs=P("ep", "tp"),
        check_vma=False,
    )
```

```python
import functools

import jax
import jax.numpy as jnp
from jax import lax
from jax.experimental import pallas as pl
from jax.experimental.pallas import tpu as pltpu
from jax.sharding import PartitionSpec as P

EPSILON = 1e-06
F32 = jnp.float32
BF16 = jnp.bfloat16
I32 = jnp.int32
MESH = pl.DeviceIdType.MESH


def layer(
    experts, tp, groups, fold, slots,
    stream_hbm, gain_hbm, chosen_hbm, aff_hbm, wg_hbm, wu_hbm, wd_hbm, fgain_hbm,
    out_ref,
    x_v, xn_v, gain_v, gainf_v, chosen_v, aff_v, fgain_v, wg_v, wu_v, wd_v,
    sel_v, place_v, pack_v, spread_v, affc_v,
    send_v, recv_v, piece_v, accg_v, accu_v, hidden_v,
    psend_v, pown_v, prec_v, ysend_v, yrec_v, leave_v, ret_v, merged_v, ssq_v,
    x_sem, s_sem, wg_sem, wu_sem, wd_sem,
    dsend, drecv, gsend, grecv, fsend, frecv, psend, precv, ysend, yrecv,
    rsend, rrecv, qsend, qrecv,
):
    me = lax.axis_index("ep")
    col = lax.axis_index("tp")
    tok, width = x_v.shape
    share = width // tp
    fw = share // fold
    caps = chosen_v.shape[1]
    cg = caps // groups
    sg = slots // groups
    mr = sg * fold
    rows = experts * mr
    chips = tp // 2
    y = col // 2
    core = col % 2
    partner = y * 2 + 1 - core

    barrier = pltpu.get_barrier_semaphore()
    for r in range(1, experts):
        pl.semaphore_signal(barrier, inc=1, device_id={"ep": (me + r) % experts, "tp": partner}, device_id_type=MESH)
    for r in range(1, tp):
        pl.semaphore_signal(barrier, inc=1, device_id={"tp": (col + r) % tp}, device_id_type=MESH)

    gather_cols = [col, partner]
    scatter_cols = [partner, col]
    for r in range(1, chips):
        before = (y + chips - r) % chips * 2
        after = (y + r) % chips * 2
        gather_cols += [before + 1 - core, before + core]
        scatter_cols += [after + core, after + 1 - core]

    small = []
    for n, (src, dst) in enumerate(
        ((chosen_hbm, chosen_v), (gain_hbm, gain_v), (aff_hbm, aff_v), (fgain_hbm, fgain_v))
    ):
        copy = pltpu.make_async_copy(src, dst, s_sem.at[n])
        copy.start()
        small.append(copy)
    pieces = x_sem.shape[0]
    xrows = tok // pieces
    x_copies = []
    for i in range(pieces):
        at = pl.ds(i * xrows, xrows)
        copy = pltpu.make_async_copy(stream_hbm.at[at, :], x_v.at[at, :], x_sem.at[i])
        copy.start()
        x_copies.append(copy)

    small[0].wait()
    base = (me * tok).astype(F32)
    lane_cap = lax.broadcasted_iota(I32, (mr, caps), 1)
    lane_tok = lax.broadcasted_iota(I32, (mr, tok), 1).astype(F32)
    sub = lax.broadcasted_iota(I32, (mr, 1), 0)
    sub_half = sum((jnp.where(sub >= h * sg, 1, 0) for h in range(1, fold)), jnp.zeros((mr, 1), I32))
    sub_slot = sub - sg * sub_half

    def build_sel(e, carry):
        row = chosen_v[pl.ds(e, 1), :].astype(F32)
        start = jnp.sum(jnp.where(row < base, 1.0, 0.0), axis=1, keepdims=True).astype(I32)
        for g in range(groups):
            first = start + ((g - start) & (groups - 1))
            hit = lane_cap == first + groups * sub_slot
            token = jnp.sum(jnp.where(hit, row + 1.0, 0.0), axis=1, keepdims=True) - 1.0 - base
            for h in range(fold):
                one = (token == lane_tok) & (sub_half == h)
                sel_v[g, e, :, h * tok:(h + 1) * tok] = jnp.where(one, 1.0, 0.0).astype(BF16)
        return carry

    lax.fori_loop(0, experts, build_sel, 0, unroll=experts <= 8)

    small[1].wait()
    gainf_v[...] = gain_v[...].astype(F32)
    lines = share // 128
    gain = jnp.concatenate(
        [gainf_v[pl.ds(partner * lines + i, 1), :] for i in range(lines)], axis=1
    )
    step = 32
    for i in range(pieces):
        x_copies[i].wait()
        if i == pieces - 1:
            for s, frm in enumerate(gather_cols):
                for src, dst, sem in ((wg_hbm, wg_v, wg_sem), (wu_hbm, wu_v, wu_sem)):
                    pltpu.make_async_copy(
                        src.at[pl.ds(frm * share, share), :],
                        dst.at[pl.ds(s * share, share), :],
                        sem.at[0 if s < 2 else 1 + s % 2],
                    ).start()
            for s, to in enumerate(scatter_cols):
                pltpu.make_async_copy(
                    wd_hbm.at[:, pl.ds(pl.multiple_of(to * share, 128), share)],
                    wd_v.at[s], wd_sem,
                ).start()
        for b in range(xrows // step):
            at = pl.ds(i * xrows + b * step, step)
            block = x_v[at, :].astype(F32)
            scale = lax.rsqrt(jnp.sum(block * block, axis=1, keepdims=True) / width + EPSILON)
            own = x_v[at, pl.ds(pl.multiple_of(partner * share, 128), share)].astype(F32)
            normed = (own * scale * gain).astype(BF16)
            for h in range(fold):
                xn_v[pl.ds(h * tok + i * xrows + b * step, step), :] = normed[:, h * fw:(h + 1) * fw]

    far_first = sorted(range(experts), key=lambda r: -min(r, experts - r))

    def exchange(g, src, dst, ssem, rsem):
        for r in far_first:
            to = (me + r) % experts
            pltpu.make_async_remote_copy(
                src_ref=src.at[g, to], dst_ref=dst.at[g, me],
                send_sem=ssem, recv_sem=rsem.at[g],
                device_id={"ep": to, "tp": partner}, device_id_type=MESH,
            ).start()

    def remote_wait(ref, sem):
        pltpu.make_async_copy(ref, ref, sem).wait()

    for g in range(groups):
        out = jnp.dot(sel_v[g].reshape(rows, fold * tok), xn_v[...], preferred_element_type=F32)
        send_v[g] = out.astype(BF16).reshape(experts, mr, fw)
        if g == 0:
            pl.semaphore_wait(barrier, experts - 1 + tp - 1)
        exchange(g, send_v, recv_v, dsend, drecv)

    own_row = chosen_v[pl.ds(me, 1), :].astype(F32)

    def positions(axis):
        shape = (rows, 1) if axis == 0 else (1, rows)
        j = lax.broadcasted_iota(I32, shape, axis)
        start = jnp.zeros(shape, F32)
        end = jnp.zeros(shape, F32)
        within = j
        cut = jnp.zeros((1, 1), F32)
        for d in range(experts):
            mine = (j >= d * mr) & (j < (d + 1) * mr)
            after = jnp.sum(jnp.where(own_row < float((d + 1) * tok), 1.0, 0.0), axis=1, keepdims=True)
            start = start + jnp.where(mine, cut, 0.0)
            end = end + jnp.where(mine, after, 0.0)
            within = within - jnp.where(mine, d * mr, 0)
            cut = after
        half = sum((jnp.where(within >= h * sg, 1, 0) for h in range(1, fold)), jnp.zeros(shape, I32))
        return start.astype(I32), end.astype(I32), half, within - sg * half

    for axis, dst in ((1, pack_v), (0, spread_v)):
        start, end, half, slot = positions(axis)
        for g in range(groups):
            want = start + ((g - start) & (groups - 1)) + groups * slot
            want = jnp.where(want < end, want, -1)
            for h in range(fold):
                aim = jnp.where(half == h, want, -1)
                if axis == 1:
                    pick = lax.broadcasted_iota(I32, (cg, rows), 0) * groups + g
                    pack_v[g, h * cg:(h + 1) * cg, :] = jnp.where(pick == aim, 1.0, 0.0).astype(BF16)
                else:
                    pick = lax.broadcasted_iota(I32, (rows, cg), 1) * groups + g
                    spread_v[g, :, h * cg:(h + 1) * cg] = jnp.where(pick == aim, 1.0, 0.0).astype(BF16)

    small[2].wait()
    for g in range(groups):
        lane = lax.broadcasted_iota(I32, (cg, caps), 1)
        pick = lax.broadcasted_iota(I32, (cg, caps), 0) * groups + g
        affc_v[g] = jnp.sum(jnp.where(lane == pick, aff_v[...], 0.0), axis=1, keepdims=True)

    for g in range(groups):
        whole = sel_v[g].reshape(rows, fold * tok).astype(F32)
        place_v[g] = whole.T.astype(BF16)

    def gather_start(g):
        remote_wait(recv_v.at[g], drecv.at[g])
        got = recv_v[g].reshape(rows, fw)
        piece_v[g, 0] = jnp.dot(pack_v[g], got, preferred_element_type=F32).astype(BF16)
        for r in range(1, chips):
            pltpu.make_async_remote_copy(
                src_ref=piece_v.at[g, 0], dst_ref=piece_v.at[g, 2 * r],
                send_sem=gsend, recv_sem=grecv.at[g],
                device_id={"tp": (y + r) % chips * 2 + 1 - core}, device_id_type=MESH,
            ).start()
        forward(g, 0)

    def forward(g, r):
        pltpu.make_async_remote_copy(
            src_ref=piece_v.at[g, 2 * r], dst_ref=piece_v.at[g, 2 * r + 1],
            send_sem=fsend, recv_sem=frecv.at[g, min(r, 1)],
            device_id={"tp": partner}, device_id_type=MESH,
        ).start()

    def gather_forward(g):
        remote_wait(piece_v.at[g, pl.ds(0, chips - 1)], grecv.at[g])
        for r in range(1, chips):
            forward(g, r)

    waited = set()

    def weight_wait(n):
        if n not in waited:
            waited.add(n)
            if n == 3:
                remote_wait(wd_v, wd_sem)
            else:
                at = pl.ds(0, (2 if n == 0 else chips - 1) * share)
                remote_wait(wg_v.at[at, :], wg_sem.at[n])
                remote_wait(wu_v.at[at, :], wu_sem.at[n])

    def contract(g, slots_in):
        taken = jnp.concatenate(
            [piece_v[g, s, h * cg:(h + 1) * cg, :] for s in slots_in for h in range(fold)], axis=1
        )
        if slots_in == [0, 1]:
            return [
                jnp.dot(taken, w[0:2 * share, :], preferred_element_type=F32) for w in (wg_v, wu_v)
            ]
        return [
            sum(
                jnp.dot(
                    taken[:, n * share:(n + 1) * share], w[s * share:(s + 1) * share, :],
                    preferred_element_type=F32,
                )
                for n, s in enumerate(slots_in)
            )
            for w in (wg_v, wu_v)
        ]

    def near(g):
        remote_wait(piece_v.at[g, 1], frecv.at[g, 0])
        weight_wait(0)
        accg_v[g], accu_v[g] = contract(g, [0, 1])

    def middle(g):
        weight_wait(1)
        gate, up = contract(g, [2 * r for r in range(1, chips)])
        accg_v[g] += gate
        accu_v[g] += up

    def away(g):
        remote_wait(piece_v.at[g, pl.ds(0, chips - 1)], frecv.at[g, 1])
        weight_wait(2)
        gate, up = contract(g, [2 * r + 1 for r in range(1, chips)])
        gate = gate + accg_v[g]
        up = up + accu_v[g]
        hidden_v[g] = (gate / (1.0 + jnp.exp(-gate)) * up).astype(BF16)
        weight_wait(3)
        for r in range(1, chips):
            pair(g, r)

    def down(g, s):
        return jnp.dot(hidden_v[g], wd_v[s], preferred_element_type=F32)

    def pair(g, r):
        psend_v[g, r] = down(g, 2 * r + 1).astype(BF16)
        pltpu.make_async_remote_copy(
            src_ref=psend_v.at[g, r], dst_ref=prec_v.at[g, r],
            send_sem=psend, recv_sem=precv.at[g, min(r, 1)],
            device_id={"tp": partner}, device_id_type=MESH,
        ).start()

    def home(g):
        for r in range(1, chips):
            pown_v[g, r] = down(g, 2 * r)
        pair(g, 0)

    def cross(g):
        remote_wait(prec_v.at[g, pl.ds(0, chips - 1)], precv.at[g, 1])
        for r in range(1, chips):
            ysend_v[g, r] = (pown_v[g, r] + prec_v[g, r].astype(F32)).astype(BF16)
            pltpu.make_async_remote_copy(
                src_ref=ysend_v.at[g, r], dst_ref=yrec_v.at[g, r],
                send_sem=ysend, recv_sem=yrecv.at[g],
                device_id={"tp": (y + r) % chips * 2 + 1 - core}, device_id_type=MESH,
            ).start()
        pown_v[g, 0] = down(g, 0)

    def leave(g):
        remote_wait(prec_v.at[g, 0], precv.at[g, 0])
        total = pown_v[g, 0] + prec_v[g, 0].astype(F32)
        remote_wait(yrec_v.at[g, pl.ds(0, chips - 1)], yrecv.at[g])
        for r in range(1, chips):
            total = total + yrec_v[g, r].astype(F32)
        weighted = (total * affc_v[g]).astype(BF16)
        folded = jnp.concatenate([weighted[:, h * fw:(h + 1) * fw] for h in range(fold)], axis=0)
        out = jnp.dot(spread_v[g], folded, preferred_element_type=F32)
        leave_v[g] = out.astype(BF16).reshape(experts, mr, fw)
        exchange(g, leave_v, ret_v, rsend, rrecv)

    def settle(g):
        remote_wait(ret_v.at[g], rrecv.at[g])
        update = jnp.dot(place_v[g], ret_v[g].reshape(rows, fw), preferred_element_type=F32)
        if g == 0:
            for h in range(fold):
                at = pl.ds(pl.multiple_of(col * share + h * fw, 128), fw)
                merged_v[h * tok:(h + 1) * tok, :] = x_v[:, at].astype(F32) + update[h * tok:(h + 1) * tok, :]
        else:
            merged_v[...] = merged_v[...] + update

    stages = {
        "s1": gather_start, "s2": gather_forward, "a": near, "m": middle, "b": away, "h": home,
        "x": cross, "l": leave, "r": settle,
    }
    if groups == 4:
        order = ORDER4
    else:
        order = [f"{name}.{g}" for name in ("s1", "s2", "a", "m", "b", "h", "x", "l", "r") for g in range(groups)]
    for item in order:
        name, g = item.split(".")
        with jax.named_scope(name + g):
            stages[name](int(g))

    square = 128
    eye = (
        lax.broadcasted_iota(I32, (square, square), 0)
        == lax.broadcasted_iota(I32, (square, square), 1)
    )
    merged = merged_v[...]
    both = jnp.sum(merged * merged, axis=1, keepdims=True)
    squares = both[0:tok]
    for h in range(1, fold):
        squares = squares + both[h * tok:(h + 1) * tok]
    for b in range(tok // square):
        line = jnp.sum(
            jnp.where(eye, squares[b * square:(b + 1) * square, :], 0.0), axis=0, keepdims=True
        )
        ssq_v[0, :, b * square:(b + 1) * square] = jnp.broadcast_to(line, (8, square))

    def square_copy(r):
        return pltpu.make_async_remote_copy(
            src_ref=ssq_v.at[0], dst_ref=ssq_v.at[r],
            send_sem=qsend, recv_sem=qrecv,
            device_id={"tp": (col + r) % tp}, device_id_type=MESH,
        )

    for r in range(1, tp):
        square_copy(r).start()
    small[3].wait()
    closing = fgain_v[...].astype(F32)
    fgain = jnp.concatenate([closing[i:i + 1, :] for i in range(lines)], axis=1)
    sums = ssq_v[0]
    with jax.named_scope("sqw"):
        remote_wait(ssq_v.at[pl.ds(1, tp - 1)], qrecv)
        for r in range(1, tp):
            sums = sums + ssq_v[r]
    scales = lax.rsqrt(sums[0:1, :] / width + EPSILON)
    for b in range(tok // square):
        line = scales[:, b * square:(b + 1) * square]
        column = jnp.sum(jnp.where(eye, line, 0.0), axis=1, keepdims=True)
        for h in range(fold):
            part = merged_v[h * tok + b * square:h * tok + (b + 1) * square, :]
            out_ref[b * square:(b + 1) * square, h * fw:(h + 1) * fw] = (
                part * column * fgain[:, h * fw:(h + 1) * fw]
            ).astype(BF16)

    with jax.named_scope("fin"):
        remote_wait(send_v, dsend)
        remote_wait(piece_v.at[:, pl.ds(0, chips - 1)], gsend)
        remote_wait(piece_v.at[:, pl.ds(0, chips)], fsend)
        remote_wait(psend_v, psend)
        remote_wait(ysend_v.at[:, pl.ds(0, chips - 1)], ysend)
        remote_wait(leave_v, rsend)
        remote_wait(ssq_v.at[pl.ds(1, tp - 1)], qsend)


ORDER4 = [
    "s1.0", "a.0", "s1.1", "s2.0", "m.0", "a.1", "b.0", "h.0", "s1.2", "s2.1", "x.0", "m.1", "a.2", "b.1", "h.1",
    "s1.3", "s2.2", "x.1", "m.2", "l.0", "b.2", "h.2", "a.3", "x.2", "s2.3", "m.3", "l.1", "b.3", "h.3",
    "x.3", "l.2", "r.0", "l.3", "r.1", "r.2", "r.3",
]


def on_device(stream, ffn_gain, chosen, affinity, w_gate, w_up, w_down, final_gain):
    tok, width = stream.shape
    experts, caps = chosen.shape
    tp = lax.axis_size("tp")
    share = width // tp
    hid = w_gate.shape[2]
    slots = 3 * tok // 16
    groups, fold = (4, 2) if share % 256 == 0 else (2, 1)
    fw = share // fold
    cg = caps // groups
    mr = slots // groups * fold
    rows = experts * mr
    chips = tp // 2
    hbm = pl.BlockSpec(memory_space=pltpu.HBM)
    dma = pltpu.SemaphoreType.DMA
    buffers = [
        pltpu.VMEM((tok, width), BF16),
        pltpu.VMEM((fold * tok, fw), BF16),
        pltpu.VMEM((width // 128, 128), BF16),
        pltpu.VMEM((width // 128, 128), F32),
        pltpu.VMEM((experts, caps), I32),
        pltpu.VMEM((1, caps), F32),
        pltpu.VMEM((share // 128, 128), BF16),
        pltpu.VMEM((width, hid), BF16),
        pltpu.VMEM((width, hid), BF16),
        pltpu.VMEM((tp, hid, share), BF16),
        pltpu.VMEM((groups, experts, mr, fold * tok), BF16),
        pltpu.VMEM((groups, fold * tok, rows), BF16),
        pltpu.VMEM((groups, fold * cg, rows), BF16),
        pltpu.VMEM((groups, rows, fold * cg), BF16),
        pltpu.VMEM((groups, cg, 1), F32),
        pltpu.VMEM((groups, experts, mr, fw), BF16),
        pltpu.VMEM((groups, experts, mr, fw), BF16),
        pltpu.VMEM((groups, tp, fold * cg, fw), BF16),
        pltpu.VMEM((groups, cg, hid), F32),
        pltpu.VMEM((groups, cg, hid), F32),
        pltpu.VMEM((groups, cg, hid), BF16),
        pltpu.VMEM((groups, chips, cg, share), BF16),
        pltpu.VMEM((groups, chips, cg, share), F32),
        pltpu.VMEM((groups, chips, cg, share), BF16),
        pltpu.VMEM((groups, chips, cg, share), BF16),
        pltpu.VMEM((groups, chips, cg, share), BF16),
        pltpu.VMEM((groups, experts, mr, fw), BF16),
        pltpu.VMEM((groups, experts, mr, fw), BF16),
        pltpu.VMEM((fold * tok, fw), F32),
        pltpu.VMEM((tp, 8, tok), F32),
    ]
    return pl.pallas_call(
        functools.partial(layer, experts, tp, groups, fold, slots),
        out_shape=pltpu.VMEM((tok, share), BF16),
        in_specs=[hbm] * 8,
        out_specs=pl.BlockSpec(memory_space=pltpu.VMEM),
        scratch_shapes=buffers + [
            dma((4,)), dma((4,)), dma((3,)), dma((3,)), dma,
            dma, dma((groups,)), dma, dma((groups,)), dma, dma((groups, 2)),
            dma, dma((groups, 2)), dma, dma((groups,)), dma, dma((groups,)), dma, dma,
        ],
        compiler_params=pltpu.CompilerParams(
            collective_id=0, has_side_effects=True, vmem_limit_bytes=56 * 1024 * 1024
        ),
        name="layer",
    )(
        stream,
        ffn_gain.reshape(width // 128, 128),
        chosen,
        affinity,
        w_gate[0],
        w_up[0],
        w_down[0],
        final_gain.reshape(share // 128, 128),
    )


def solution(mesh):
    return jax.shard_map(
        on_device,
        mesh=mesh,
        in_specs=(
            P("ep", None),
            P(),
            P(),
            P("ep", None),
            P("ep", None, "tp"),
            P("ep", None, "tp"),
            P("ep", "tp", None),
            P("tp"),
        ),
        out_specs=P("ep", "tp"),
        check_vma=False,
    )
```

```python
import functools

import jax
import jax.numpy as jnp
from jax import lax
from jax.experimental import pallas as pl
from jax.experimental.pallas import tpu as pltpu
from jax.sharding import PartitionSpec as P

EPSILON = 1e-06
F32 = jnp.float32
BF16 = jnp.bfloat16
I32 = jnp.int32
MESH = pl.DeviceIdType.MESH


def layer(
    experts, tp, groups, fold, slots,
    stream_hbm, gain_hbm, chosen_hbm, aff_hbm, wg_hbm, wu_hbm, wd_hbm, fgain_hbm,
    out_ref,
    x_v, xn_v, gain_v, gainf_v, chosen_v, aff_v, fgain_v, wg_v, wu_v, wd_v,
    sel_v, place_v, pack_v, spread_v, affc_v,
    send_v, recv_v, piece_v, accg_v, accu_v, hidden_v,
    psend_v, pown_v, prec_v, ysend_v, yrec_v, leave_v, ret_v, merged_v, ssq_v,
    x_sem, s_sem, wg_sem, wu_sem, wd_sem,
    dsend, drecv, gsend, grecv, fsend, frecv, psend, precv, ysend, yrecv,
    rsend, rrecv, qsend, qrecv,
):
    me = lax.axis_index("ep")
    col = lax.axis_index("tp")
    tok, width = x_v.shape
    share = width // tp
    fw = share // fold
    caps = chosen_v.shape[1]
    cg = caps // groups
    sg = slots // groups
    mr = sg * fold
    rows = experts * mr
    chips = tp // 2
    y = col // 2
    core = col % 2
    partner = y * 2 + 1 - core

    barrier = pltpu.get_barrier_semaphore()
    for r in range(1, experts):
        pl.semaphore_signal(barrier, inc=1, device_id={"ep": (me + r) % experts, "tp": partner}, device_id_type=MESH)
    for r in range(1, tp):
        pl.semaphore_signal(barrier, inc=1, device_id={"tp": (col + r) % tp}, device_id_type=MESH)

    gather_cols = [col, partner]
    scatter_cols = [partner, col]
    for r in range(1, chips):
        before = (y + chips - r) % chips * 2
        after = (y + r) % chips * 2
        gather_cols += [before + 1 - core, before + core]
        scatter_cols += [after + core, after + 1 - core]

    small = []
    for n, (src, dst) in enumerate(
        ((chosen_hbm, chosen_v), (gain_hbm, gain_v), (aff_hbm, aff_v), (fgain_hbm, fgain_v))
    ):
        copy = pltpu.make_async_copy(src, dst, s_sem.at[n])
        copy.start()
        small.append(copy)
    pieces = x_sem.shape[0]
    xrows = tok // pieces
    x_copies = []
    for i in range(pieces):
        at = pl.ds(i * xrows, xrows)
        copy = pltpu.make_async_copy(stream_hbm.at[at, :], x_v.at[at, :], x_sem.at[i])
        copy.start()
        x_copies.append(copy)

    small[0].wait()
    base = (me * tok).astype(F32)
    lane_cap = lax.broadcasted_iota(I32, (mr, caps), 1)
    lane_tok = lax.broadcasted_iota(I32, (mr, tok), 1).astype(F32)
    sub = lax.broadcasted_iota(I32, (mr, 1), 0)
    sub_half = sum((jnp.where(sub >= h * sg, 1, 0) for h in range(1, fold)), jnp.zeros((mr, 1), I32))
    sub_slot = sub - sg * sub_half

    def build_sel(g):
        def one_expert(e, carry):
            row = chosen_v[pl.ds(e, 1), :].astype(F32)
            start = jnp.sum(jnp.where(row < base, 1.0, 0.0), axis=1, keepdims=True).astype(I32)
            first = start + ((g - start) & (groups - 1))
            hit = lane_cap == first + groups * sub_slot
            token = jnp.sum(jnp.where(hit, row + 1.0, 0.0), axis=1, keepdims=True) - 1.0 - base
            for h in range(fold):
                one = (token == lane_tok) & (sub_half == h)
                sel_v[g, e, :, h * tok:(h + 1) * tok] = jnp.where(one, 1.0, 0.0).astype(BF16)
            return carry

        lax.fori_loop(0, experts, one_expert, 0, unroll=experts <= 8)

    build_sel(0)
    small[1].wait()
    gainf_v[...] = gain_v[...].astype(F32)
    lines = share // 128
    gain = jnp.concatenate(
        [gainf_v[pl.ds(partner * lines + i, 1), :] for i in range(lines)], axis=1
    )
    step = 32
    for i in range(pieces):
        x_copies[i].wait()
        if i == pieces - 1:
            for s, frm in enumerate(gather_cols):
                for src, dst, sem in ((wg_hbm, wg_v, wg_sem), (wu_hbm, wu_v, wu_sem)):
                    pltpu.make_async_copy(
                        src.at[pl.ds(frm * share, share), :],
                        dst.at[pl.ds(s * share, share), :],
                        sem.at[0 if s < 2 else 1 + s % 2],
                    ).start()
            for s, to in enumerate(scatter_cols):
                pltpu.make_async_copy(
                    wd_hbm.at[:, pl.ds(pl.multiple_of(to * share, 128), share)],
                    wd_v.at[s], wd_sem,
                ).start()
        for b in range(xrows // step):
            at = pl.ds(i * xrows + b * step, step)
            block = x_v[at, :].astype(F32)
            scale = lax.rsqrt(jnp.sum(block * block, axis=1, keepdims=True) / width + EPSILON)
            own = x_v[at, pl.ds(pl.multiple_of(partner * share, 128), share)].astype(F32)
            normed = (own * scale * gain).astype(BF16)
            for h in range(fold):
                xn_v[pl.ds(h * tok + i * xrows + b * step, step), :] = normed[:, h * fw:(h + 1) * fw]

    far_first = sorted(range(experts), key=lambda r: -min(r, experts - r))
    half_n = experts // 2
    side = me // half_n

    def target(i):
        if i < half_n:
            return (1 - side) * half_n + (me + i) % half_n
        return side * half_n + (me + i + 1) % half_n

    def exchange(g, src, dst, ssem, rsem):
        for i in range(experts):
            to = (me + far_first[i]) % experts
            pltpu.make_async_remote_copy(
                src_ref=src.at[g, to], dst_ref=dst.at[g, me],
                send_sem=ssem, recv_sem=rsem.at[g],
                device_id={"ep": to, "tp": partner}, device_id_type=MESH,
            ).start()

    def remote_wait(ref, sem):
        pltpu.make_async_copy(ref, ref, sem).wait()

    window = 2
    for g in range(groups):
        if g > 0:
            build_sel(g)
        out = jnp.dot(sel_v[g].reshape(rows, fold * tok), xn_v[...], preferred_element_type=F32)
        send_v[g] = out.astype(BF16).reshape(experts, mr, fw)
        if g == 0:
            pl.semaphore_wait(barrier, experts - 1 + tp - 1)
        if g < window:
            exchange(g, send_v, recv_v, dsend, drecv)

    own_row = chosen_v[pl.ds(me, 1), :].astype(F32)

    def positions(axis):
        shape = (rows, 1) if axis == 0 else (1, rows)
        j = lax.broadcasted_iota(I32, shape, axis)
        start = jnp.zeros(shape, F32)
        end = jnp.zeros(shape, F32)
        within = j
        cut = jnp.zeros((1, 1), F32)
        for d in range(experts):
            mine = (j >= d * mr) & (j < (d + 1) * mr)
            after = jnp.sum(jnp.where(own_row < float((d + 1) * tok), 1.0, 0.0), axis=1, keepdims=True)
            start = start + jnp.where(mine, cut, 0.0)
            end = end + jnp.where(mine, after, 0.0)
            within = within - jnp.where(mine, d * mr, 0)
            cut = after
        half = sum((jnp.where(within >= h * sg, 1, 0) for h in range(1, fold)), jnp.zeros(shape, I32))
        return start.astype(I32), end.astype(I32), half, within - sg * half

    for axis, dst in ((1, pack_v), (0, spread_v)):
        start, end, half, slot = positions(axis)
        for g in range(groups):
            want = start + ((g - start) & (groups - 1)) + groups * slot
            want = jnp.where(want < end, want, -1)
            for h in range(fold):
                aim = jnp.where(half == h, want, -1)
                if axis == 1:
                    pick = lax.broadcasted_iota(I32, (cg, rows), 0) * groups + g
                    pack_v[g, h * cg:(h + 1) * cg, :] = jnp.where(pick == aim, 1.0, 0.0).astype(BF16)
                else:
                    pick = lax.broadcasted_iota(I32, (rows, cg), 1) * groups + g
                    spread_v[g, :, h * cg:(h + 1) * cg] = jnp.where(pick == aim, 1.0, 0.0).astype(BF16)

    small[2].wait()
    for g in range(groups):
        lane = lax.broadcasted_iota(I32, (cg, caps), 1)
        pick = lax.broadcasted_iota(I32, (cg, caps), 0) * groups + g
        affc_v[g] = jnp.sum(jnp.where(lane == pick, aff_v[...], 0.0), axis=1, keepdims=True)

    for g in range(groups):
        whole = sel_v[g].reshape(rows, fold * tok).astype(F32)
        place_v[g] = whole.T.astype(BF16)

    def gather_start(g):
        remote_wait(recv_v.at[g], drecv.at[g])
        if g + window < groups:
            exchange(g + window, send_v, recv_v, dsend, drecv)
        got = recv_v[g].reshape(rows, fw)
        piece_v[g, 0] = jnp.dot(pack_v[g], got, preferred_element_type=F32).astype(BF16)
        for r in range(1, chips):
            pltpu.make_async_remote_copy(
                src_ref=piece_v.at[g, 0], dst_ref=piece_v.at[g, 2 * r],
                send_sem=gsend, recv_sem=grecv.at[g],
                device_id={"tp": (y + r) % chips * 2 + 1 - core}, device_id_type=MESH,
            ).start()
        forward(g, 0)

    def forward(g, r):
        pltpu.make_async_remote_copy(
            src_ref=piece_v.at[g, 2 * r], dst_ref=piece_v.at[g, 2 * r + 1],
            send_sem=fsend, recv_sem=frecv.at[g, min(r, 1)],
            device_id={"tp": partner}, device_id_type=MESH,
        ).start()

    def gather_forward(g):
        remote_wait(piece_v.at[g, pl.ds(0, chips - 1)], grecv.at[g])
        for r in range(1, chips):
            forward(g, r)

    waited = set()

    def weight_wait(n):
        if n not in waited:
            waited.add(n)
            if n == 3:
                remote_wait(wd_v, wd_sem)
            else:
                at = pl.ds(0, (2 if n == 0 else chips - 1) * share)
                remote_wait(wg_v.at[at, :], wg_sem.at[n])
                remote_wait(wu_v.at[at, :], wu_sem.at[n])

    def contract(g, slots_in):
        taken = jnp.concatenate(
            [piece_v[g, s, h * cg:(h + 1) * cg, :] for s in slots_in for h in range(fold)], axis=1
        )
        if slots_in == [0, 1]:
            return [
                jnp.dot(taken, w[0:2 * share, :], preferred_element_type=F32) for w in (wg_v, wu_v)
            ]
        return [
            sum(
                jnp.dot(
                    taken[:, n * share:(n + 1) * share], w[s * share:(s + 1) * share, :],
                    preferred_element_type=F32,
                )
                for n, s in enumerate(slots_in)
            )
            for w in (wg_v, wu_v)
        ]

    def near(g):
        remote_wait(piece_v.at[g, 1], frecv.at[g, 0])
        weight_wait(0)
        accg_v[g], accu_v[g] = contract(g, [0, 1])

    def middle(g):
        weight_wait(1)
        gate, up = contract(g, [2 * r for r in range(1, chips)])
        accg_v[g] += gate
        accu_v[g] += up

    def away(g):
        remote_wait(piece_v.at[g, pl.ds(0, chips - 1)], frecv.at[g, 1])
        weight_wait(2)
        gate, up = contract(g, [2 * r + 1 for r in range(1, chips)])
        gate = gate + accg_v[g]
        up = up + accu_v[g]
        hidden_v[g] = (gate / (1.0 + jnp.exp(-gate)) * up).astype(BF16)
        weight_wait(3)
        for r in range(1, chips):
            pair(g, r)

    def down(g, s):
        return jnp.dot(hidden_v[g], wd_v[s], preferred_element_type=F32)

    def pair(g, r):
        psend_v[g, r] = down(g, 2 * r + 1).astype(BF16)
        pltpu.make_async_remote_copy(
            src_ref=psend_v.at[g, r], dst_ref=prec_v.at[g, r],
            send_sem=psend, recv_sem=precv.at[g, min(r, 1)],
            device_id={"tp": partner}, device_id_type=MESH,
        ).start()

    def home(g):
        for r in range(1, chips):
            pown_v[g, r] = down(g, 2 * r)
        pair(g, 0)

    def cross(g):
        remote_wait(prec_v.at[g, pl.ds(0, chips - 1)], precv.at[g, 1])
        for r in range(1, chips):
            ysend_v[g, r] = (pown_v[g, r] + prec_v[g, r].astype(F32)).astype(BF16)
            pltpu.make_async_remote_copy(
                src_ref=ysend_v.at[g, r], dst_ref=yrec_v.at[g, r],
                send_sem=ysend, recv_sem=yrecv.at[g],
                device_id={"tp": (y + r) % chips * 2 + 1 - core}, device_id_type=MESH,
            ).start()
        pown_v[g, 0] = down(g, 0)

    def leave(g):
        remote_wait(prec_v.at[g, 0], precv.at[g, 0])
        total = pown_v[g, 0] + prec_v[g, 0].astype(F32)
        remote_wait(yrec_v.at[g, pl.ds(0, chips - 1)], yrecv.at[g])
        for r in range(1, chips):
            total = total + yrec_v[g, r].astype(F32)
        weighted = (total * affc_v[g]).astype(BF16)
        folded = jnp.concatenate([weighted[:, h * fw:(h + 1) * fw] for h in range(fold)], axis=0)
        out = jnp.dot(spread_v[g], folded, preferred_element_type=F32)
        leave_v[g] = out.astype(BF16).reshape(experts, mr, fw)
        exchange(g, leave_v, ret_v, rsend, rrecv)

    def settle(g):
        remote_wait(ret_v.at[g], rrecv.at[g])
        update = jnp.dot(place_v[g], ret_v[g].reshape(rows, fw), preferred_element_type=F32)
        if g == 0:
            for h in range(fold):
                at = pl.ds(pl.multiple_of(col * share + h * fw, 128), fw)
                merged_v[h * tok:(h + 1) * tok, :] = x_v[:, at].astype(F32) + update[h * tok:(h + 1) * tok, :]
        else:
            merged_v[...] = merged_v[...] + update

    stages = {
        "s1": gather_start, "s2": gather_forward, "a": near, "m": middle, "b": away, "h": home,
        "x": cross, "l": leave, "r": settle,
    }
    if groups == 4:
        order = ORDER4
    else:
        order = [f"{name}.{g}" for name in ("s1", "s2", "a", "m", "b", "h", "x", "l", "r") for g in range(groups)]
    for item in order:
        name, g = item.split(".")
        with jax.named_scope(name + g):
            stages[name](int(g))

    square = 128
    eye = (
        lax.broadcasted_iota(I32, (square, square), 0)
        == lax.broadcasted_iota(I32, (square, square), 1)
    )
    merged = merged_v[...]
    both = jnp.sum(merged * merged, axis=1, keepdims=True)
    squares = both[0:tok]
    for h in range(1, fold):
        squares = squares + both[h * tok:(h + 1) * tok]
    for b in range(tok // square):
        line = jnp.sum(
            jnp.where(eye, squares[b * square:(b + 1) * square, :], 0.0), axis=0, keepdims=True
        )
        ssq_v[0, :, b * square:(b + 1) * square] = jnp.broadcast_to(line, (8, square))

    def square_copy(r):
        return pltpu.make_async_remote_copy(
            src_ref=ssq_v.at[0], dst_ref=ssq_v.at[r],
            send_sem=qsend, recv_sem=qrecv,
            device_id={"tp": (col + r) % tp}, device_id_type=MESH,
        )

    for r in range(1, tp):
        square_copy(r).start()
    small[3].wait()
    closing = fgain_v[...].astype(F32)
    fgain = jnp.concatenate([closing[i:i + 1, :] for i in range(lines)], axis=1)
    sums = ssq_v[0]
    with jax.named_scope("sqw"):
        remote_wait(ssq_v.at[pl.ds(1, tp - 1)], qrecv)
        for r in range(1, tp):
            sums = sums + ssq_v[r]
    scales = lax.rsqrt(sums[0:1, :] / width + EPSILON)
    for b in range(tok // square):
        line = scales[:, b * square:(b + 1) * square]
        column = jnp.sum(jnp.where(eye, line, 0.0), axis=1, keepdims=True)
        for h in range(fold):
            part = merged_v[h * tok + b * square:h * tok + (b + 1) * square, :]
            out_ref[b * square:(b + 1) * square, h * fw:(h + 1) * fw] = (
                part * column * fgain[:, h * fw:(h + 1) * fw]
            ).astype(BF16)

    with jax.named_scope("fin"):
        remote_wait(send_v, dsend)
        remote_wait(piece_v.at[:, pl.ds(0, chips - 1)], gsend)
        remote_wait(piece_v.at[:, pl.ds(0, chips)], fsend)
        remote_wait(psend_v, psend)
        remote_wait(ysend_v.at[:, pl.ds(0, chips - 1)], ysend)
        remote_wait(leave_v, rsend)
        remote_wait(ssq_v.at[pl.ds(1, tp - 1)], qsend)


ORDER4 = [
    "s1.0", "s1.1", "a.0", "s2.0", "m.0", "b.0", "s1.2", "a.1", "h.0", "s2.1", "m.1", "x.0",
    "s1.3", "b.1", "a.2", "s2.2", "h.1", "x.1", "m.2", "a.3", "b.2", "l.0", "h.2", "s2.3",
    "m.3", "x.2", "b.3", "l.1", "h.3", "x.3", "l.2", "r.0", "l.3", "r.1", "r.2", "r.3",
]


def on_device(stream, ffn_gain, chosen, affinity, w_gate, w_up, w_down, final_gain):
    tok, width = stream.shape
    experts, caps = chosen.shape
    tp = lax.axis_size("tp")
    share = width // tp
    hid = w_gate.shape[2]
    slots = 3 * tok // 16
    groups, fold = (4, 2) if share % 256 == 0 else (2, 1)
    fw = share // fold
    cg = caps // groups
    mr = slots // groups * fold
    rows = experts * mr
    chips = tp // 2
    hbm = pl.BlockSpec(memory_space=pltpu.HBM)
    dma = pltpu.SemaphoreType.DMA
    buffers = [
        pltpu.VMEM((tok, width), BF16),
        pltpu.VMEM((fold * tok, fw), BF16),
        pltpu.VMEM((width // 128, 128), BF16),
        pltpu.VMEM((width // 128, 128), F32),
        pltpu.VMEM((experts, caps), I32),
        pltpu.VMEM((1, caps), F32),
        pltpu.VMEM((share // 128, 128), BF16),
        pltpu.VMEM((width, hid), BF16),
        pltpu.VMEM((width, hid), BF16),
        pltpu.VMEM((tp, hid, share), BF16),
        pltpu.VMEM((groups, experts, mr, fold * tok), BF16),
        pltpu.VMEM((groups, fold * tok, rows), BF16),
        pltpu.VMEM((groups, fold * cg, rows), BF16),
        pltpu.VMEM((groups, rows, fold * cg), BF16),
        pltpu.VMEM((groups, cg, 1), F32),
        pltpu.VMEM((groups, experts, mr, fw), BF16),
        pltpu.VMEM((groups, experts, mr, fw), BF16),
        pltpu.VMEM((groups, tp, fold * cg, fw), BF16),
        pltpu.VMEM((groups, cg, hid), F32),
        pltpu.VMEM((groups, cg, hid), F32),
        pltpu.VMEM((groups, cg, hid), BF16),
        pltpu.VMEM((groups, chips, cg, share), BF16),
        pltpu.VMEM((groups, chips, cg, share), F32),
        pltpu.VMEM((groups, chips, cg, share), BF16),
        pltpu.VMEM((groups, chips, cg, share), BF16),
        pltpu.VMEM((groups, chips, cg, share), BF16),
        pltpu.VMEM((groups, experts, mr, fw), BF16),
        pltpu.VMEM((groups, experts, mr, fw), BF16),
        pltpu.VMEM((fold * tok, fw), F32),
        pltpu.VMEM((tp, 8, tok), F32),
    ]
    return pl.pallas_call(
        functools.partial(layer, experts, tp, groups, fold, slots),
        out_shape=pltpu.VMEM((tok, share), BF16),
        in_specs=[hbm] * 8,
        out_specs=pl.BlockSpec(memory_space=pltpu.VMEM),
        scratch_shapes=buffers + [
            dma((2,)), dma((4,)), dma((3,)), dma((3,)), dma,
            dma, dma((groups,)), dma, dma((groups,)), dma, dma((groups, 2)),
            dma, dma((groups, 2)), dma, dma((groups,)), dma, dma((groups,)), dma, dma,
        ],
        compiler_params=pltpu.CompilerParams(
            collective_id=0, has_side_effects=True, vmem_limit_bytes=56 * 1024 * 1024
        ),
        name="layer",
    )(
        stream,
        ffn_gain.reshape(width // 128, 128),
        chosen,
        affinity,
        w_gate[0],
        w_up[0],
        w_down[0],
        final_gain.reshape(share // 128, 128),
    )


def solution(mesh):
    return jax.shard_map(
        on_device,
        mesh=mesh,
        in_specs=(
            P("ep", None),
            P(),
            P(),
            P("ep", None),
            P("ep", None, "tp"),
            P("ep", None, "tp"),
            P("ep", "tp", None),
            P("tp"),
        ),
        out_specs=P("ep", "tp"),
        check_vma=False,
    )
```

```python
import functools

import jax
import jax.numpy as jnp
from jax import lax
from jax.experimental import pallas as pl
from jax.experimental.pallas import tpu as pltpu
from jax.sharding import PartitionSpec as P

EPSILON = 1e-06
F32 = jnp.float32
BF16 = jnp.bfloat16
I32 = jnp.int32
MESH = pl.DeviceIdType.MESH


def layer(
    experts, tp, groups, fold, slots, full,
    stream_hbm, gain_hbm, chosen_hbm, aff_hbm, wg_hbm, wu_hbm, wd_hbm, fgain_hbm,
    out_ref,
    x_v, xn_v, xf_v, scale_v, gain_v, gainf_v, chosen_v, aff_v, fgain_v, wg_v, wu_v, wd_v,
    sel_v, place_v, pack_v, spread_v, affc_v,
    send_v, recv_v, sendf_v, recvf_v, piece_v, accg_v, accu_v, hidden_v,
    psend_v, pown_v, prec_v, ysend_v, yrec_v, leave_v, ret_v, merged_v, ssq_v,
    x_sem, s_sem, wg_sem, wu_sem, wd_sem,
    dsend, drecv, gsend, grecv, fsend, frecv, psend, precv, ysend, yrecv,
    rsend, rrecv, qsend, qrecv, hsend, hrecv,
):
    me = lax.axis_index("ep")
    col = lax.axis_index("tp")
    tok, width = x_v.shape
    share = width // tp
    fw = share // fold
    caps = chosen_v.shape[1]
    cg = caps // groups
    sg = slots // groups
    mr = sg * fold
    rows = experts * mr
    chips = tp // 2
    y = col // 2
    core = col % 2
    partner = y * 2 + 1 - core

    barrier = pltpu.get_barrier_semaphore()
    for r in range(1, experts):
        pl.semaphore_signal(barrier, inc=1, device_id={"ep": (me + r) % experts, "tp": partner}, device_id_type=MESH)
    for r in range(1, tp):
        pl.semaphore_signal(barrier, inc=1, device_id={"tp": (col + r) % tp}, device_id_type=MESH)

    gather_cols = [col, partner]
    scatter_cols = [partner, col]
    for r in range(1, chips):
        before = (y + chips - r) % chips * 2
        after = (y + r) % chips * 2
        gather_cols += [before + 1 - core, before + core]
        scatter_cols += [after + core, after + 1 - core]

    small = []
    for n, (src, dst) in enumerate(
        ((chosen_hbm, chosen_v), (gain_hbm, gain_v), (aff_hbm, aff_v), (fgain_hbm, fgain_v))
    ):
        copy = pltpu.make_async_copy(src, dst, s_sem.at[n])
        copy.start()
        small.append(copy)
    pieces = x_sem.shape[0]
    xrows = tok // pieces
    x_copies = []
    for i in range(pieces):
        at = pl.ds(i * xrows, xrows)
        copy = pltpu.make_async_copy(stream_hbm.at[at, :], x_v.at[at, :], x_sem.at[i])
        copy.start()
        x_copies.append(copy)

    small[0].wait()
    base = (me * tok).astype(F32)
    lane_cap = lax.broadcasted_iota(I32, (mr, caps), 1)
    lane_tok = lax.broadcasted_iota(I32, (mr, tok), 1).astype(F32)
    sub = lax.broadcasted_iota(I32, (mr, 1), 0)
    sub_half = sum((jnp.where(sub >= h * sg, 1, 0) for h in range(1, fold)), jnp.zeros((mr, 1), I32))
    sub_slot = sub - sg * sub_half

    def build_sel(g):
        def one_expert(e, carry):
            row = chosen_v[pl.ds(e, 1), :].astype(F32)
            start = jnp.sum(jnp.where(row < base, 1.0, 0.0), axis=1, keepdims=True).astype(I32)
            first = start + ((g - start) & (groups - 1))
            hit = lane_cap == first + groups * sub_slot
            token = jnp.sum(jnp.where(hit, row + 1.0, 0.0), axis=1, keepdims=True) - 1.0 - base
            for h in range(fold):
                one = (token == lane_tok) & (sub_half == h)
                sel_v[g, e, :, h * tok:(h + 1) * tok] = jnp.where(one, 1.0, 0.0).astype(BF16)
            return carry

        lax.fori_loop(0, experts, one_expert, 0, unroll=experts <= 8)

    build_sel(0)
    small[1].wait()
    gainf_v[...] = gain_v[...].astype(F32)
    lines = share // 128

    def gain_of(which):
        return jnp.concatenate(
            [gainf_v[pl.ds(which * lines + i, 1), :] for i in range(lines)], axis=1
        )

    opposite = (y + 1) % chips * 2 + 1 - core
    gain = gain_of(partner)
    step = 32
    for i in range(pieces):
        x_copies[i].wait()
        if i == pieces - 1:
            for s, frm in enumerate(gather_cols):
                for src, dst, sem in ((wg_hbm, wg_v, wg_sem), (wu_hbm, wu_v, wu_sem)):
                    pltpu.make_async_copy(
                        src.at[pl.ds(frm * share, share), :],
                        dst.at[pl.ds(s * share, share), :],
                        sem.at[0 if s < 2 else 1 + s % 2],
                    ).start()
            for s, to in enumerate(scatter_cols):
                pltpu.make_async_copy(
                    wd_hbm.at[:, pl.ds(pl.multiple_of(to * share, 128), share)],
                    wd_v.at[s], wd_sem,
                ).start()
        for b in range(xrows // step):
            at = pl.ds(i * xrows + b * step, step)
            block = x_v[at, :].astype(F32)
            scale = lax.rsqrt(jnp.sum(block * block, axis=1, keepdims=True) / width + EPSILON)
            if full:
                scale_v[at, :] = scale
            own = x_v[at, pl.ds(pl.multiple_of(partner * share, 128), share)].astype(F32)
            normed = (own * scale * gain).astype(BF16)
            for h in range(fold):
                xn_v[pl.ds(h * tok + i * xrows + b * step, step), :] = normed[:, h * fw:(h + 1) * fw]

    far_first = sorted(range(experts), key=lambda r: -min(r, experts - r))
    def exchange(g, src, dst, ssem, rsem, more=()):
        for r in far_first:
            to = (me + r) % experts
            pltpu.make_async_remote_copy(
                src_ref=src.at[g, to], dst_ref=dst.at[g, me],
                send_sem=ssem, recv_sem=rsem.at[g],
                device_id={"ep": to, "tp": partner}, device_id_type=MESH,
            ).start()
            for src_more, dst_more, ssem_more, rsem_more in more:
                pltpu.make_async_remote_copy(
                    src_ref=src_more.at[to], dst_ref=dst_more.at[me],
                    send_sem=ssem_more, recv_sem=rsem_more,
                    device_id={"ep": to, "tp": partner}, device_id_type=MESH,
                ).start()

    def dispatch(g):
        both = full and g == groups - 1
        exchange(
            g, send_v, recv_v, dsend, drecv, [(sendf_v, recvf_v, hsend, hrecv)] if both else ()
        )

    def remote_wait(ref, sem):
        pltpu.make_async_copy(ref, ref, sem).wait()

    window = 2
    for g in range(groups):
        if g > 0:
            build_sel(g)
        out = jnp.dot(sel_v[g].reshape(rows, fold * tok), xn_v[...], preferred_element_type=F32)
        send_v[g] = out.astype(BF16).reshape(experts, mr, fw)
        if full and g == groups - 1:
            gain_more = gain_of(opposite)
            for b in range(tok // step):
                at = pl.ds(b * step, step)
                own = x_v[at, pl.ds(pl.multiple_of(opposite * share, 128), share)].astype(F32)
                normed = (own * scale_v[at, :] * gain_more).astype(BF16)
                for h in range(fold):
                    xf_v[pl.ds(h * tok + b * step, step), :] = normed[:, h * fw:(h + 1) * fw]
            out = jnp.dot(sel_v[g].reshape(rows, fold * tok), xf_v[...], preferred_element_type=F32)
            sendf_v[...] = out.astype(BF16).reshape(experts, mr, fw)
        if g == 0:
            pl.semaphore_wait(barrier, experts - 1 + tp - 1)
        if g < window:
            dispatch(g)

    own_row = chosen_v[pl.ds(me, 1), :].astype(F32)

    def positions(axis):
        shape = (rows, 1) if axis == 0 else (1, rows)
        j = lax.broadcasted_iota(I32, shape, axis)
        start = jnp.zeros(shape, F32)
        end = jnp.zeros(shape, F32)
        within = j
        cut = jnp.zeros((1, 1), F32)
        for d in range(experts):
            mine = (j >= d * mr) & (j < (d + 1) * mr)
            after = jnp.sum(jnp.where(own_row < float((d + 1) * tok), 1.0, 0.0), axis=1, keepdims=True)
            start = start + jnp.where(mine, cut, 0.0)
            end = end + jnp.where(mine, after, 0.0)
            within = within - jnp.where(mine, d * mr, 0)
            cut = after
        half = sum((jnp.where(within >= h * sg, 1, 0) for h in range(1, fold)), jnp.zeros(shape, I32))
        return start.astype(I32), end.astype(I32), half, within - sg * half

    for axis, dst in ((1, pack_v), (0, spread_v)):
        start, end, half, slot = positions(axis)
        for g in range(groups):
            want = start + ((g - start) & (groups - 1)) + groups * slot
            want = jnp.where(want < end, want, -1)
            for h in range(fold):
                aim = jnp.where(half == h, want, -1)
                if axis == 1:
                    pick = lax.broadcasted_iota(I32, (cg, rows), 0) * groups + g
                    pack_v[g, h * cg:(h + 1) * cg, :] = jnp.where(pick == aim, 1.0, 0.0).astype(BF16)
                else:
                    pick = lax.broadcasted_iota(I32, (rows, cg), 1) * groups + g
                    spread_v[g, :, h * cg:(h + 1) * cg] = jnp.where(pick == aim, 1.0, 0.0).astype(BF16)

    small[2].wait()
    for g in range(groups):
        lane = lax.broadcasted_iota(I32, (cg, caps), 1)
        pick = lax.broadcasted_iota(I32, (cg, caps), 0) * groups + g
        affc_v[g] = jnp.sum(jnp.where(lane == pick, aff_v[...], 0.0), axis=1, keepdims=True)

    for g in range(groups):
        whole = sel_v[g].reshape(rows, fold * tok).astype(F32)
        place_v[g] = whole.T.astype(BF16)

    def gather_start(g):
        remote_wait(recv_v.at[g], drecv.at[g])
        if g + window < groups:
            dispatch(g + window)
        got = recv_v[g].reshape(rows, fw)
        piece_v[g, 0] = jnp.dot(pack_v[g], got, preferred_element_type=F32).astype(BF16)
        if full and g == groups - 1:
            forward(g, 0)
            remote_wait(recvf_v, hrecv)
            got = recvf_v[...].reshape(rows, fw)
            piece_v[g, 3] = jnp.dot(pack_v[g], got, preferred_element_type=F32).astype(BF16)
            pltpu.make_async_remote_copy(
                src_ref=piece_v.at[g, 3], dst_ref=piece_v.at[g, 2],
                send_sem=fsend, recv_sem=frecv.at[g, 1],
                device_id={"tp": partner}, device_id_type=MESH,
            ).start()
            return
        for r in range(1, chips):
            pltpu.make_async_remote_copy(
                src_ref=piece_v.at[g, 0], dst_ref=piece_v.at[g, 2 * r],
                send_sem=gsend, recv_sem=grecv.at[g],
                device_id={"tp": (y + r) % chips * 2 + 1 - core}, device_id_type=MESH,
            ).start()
        forward(g, 0)

    def forward(g, r):
        pltpu.make_async_remote_copy(
            src_ref=piece_v.at[g, 2 * r], dst_ref=piece_v.at[g, 2 * r + 1],
            send_sem=fsend, recv_sem=frecv.at[g, min(r, 1)],
            device_id={"tp": partner}, device_id_type=MESH,
        ).start()

    def gather_forward(g):
        remote_wait(piece_v.at[g, pl.ds(0, chips - 1)], grecv.at[g])
        for r in range(1, chips):
            forward(g, r)

    waited = set()

    def weight_wait(n):
        if n not in waited:
            waited.add(n)
            if n == 3:
                remote_wait(wd_v, wd_sem)
            else:
                at = pl.ds(0, (2 if n == 0 else chips - 1) * share)
                remote_wait(wg_v.at[at, :], wg_sem.at[n])
                remote_wait(wu_v.at[at, :], wu_sem.at[n])

    def contract(g, slots_in):
        taken = jnp.concatenate(
            [piece_v[g, s, h * cg:(h + 1) * cg, :] for s in slots_in for h in range(fold)], axis=1
        )
        if slots_in == [0, 1]:
            return [
                jnp.dot(taken, w[0:2 * share, :], preferred_element_type=F32) for w in (wg_v, wu_v)
            ]
        return [
            sum(
                jnp.dot(
                    taken[:, n * share:(n + 1) * share], w[s * share:(s + 1) * share, :],
                    preferred_element_type=F32,
                )
                for n, s in enumerate(slots_in)
            )
            for w in (wg_v, wu_v)
        ]

    def near(g):
        weight_wait(0)
        if full and g == groups - 1:
            weight_wait(2)
            accg_v[g], accu_v[g] = contract(g, [0, 3])
            return
        remote_wait(piece_v.at[g, 1], frecv.at[g, 0])
        accg_v[g], accu_v[g] = contract(g, [0, 1])

    def middle(g):
        weight_wait(1)
        gate, up = contract(g, [2 * r for r in range(1, chips)])
        accg_v[g] += gate
        accu_v[g] += up

    def away(g):
        remote_wait(piece_v.at[g, pl.ds(0, chips - 1)], frecv.at[g, 1])
        if full and g == groups - 1:
            remote_wait(piece_v.at[g, 1], frecv.at[g, 0])
            weight_wait(1)
            gate, up = contract(g, [1, 2])
        else:
            weight_wait(2)
            gate, up = contract(g, [2 * r + 1 for r in range(1, chips)])
        gate = gate + accg_v[g]
        up = up + accu_v[g]
        hidden_v[g] = (gate / (1.0 + jnp.exp(-gate)) * up).astype(BF16)
        weight_wait(3)
        for r in range(1, chips):
            pair(g, r)

    def down(g, s):
        return jnp.dot(hidden_v[g], wd_v[s], preferred_element_type=F32)

    def pair(g, r):
        psend_v[g, r] = down(g, 2 * r + 1).astype(BF16)
        pltpu.make_async_remote_copy(
            src_ref=psend_v.at[g, r], dst_ref=prec_v.at[g, r],
            send_sem=psend, recv_sem=precv.at[g, min(r, 1)],
            device_id={"tp": partner}, device_id_type=MESH,
        ).start()

    def home(g):
        for r in range(1, chips):
            pown_v[g, r] = down(g, 2 * r)
        pair(g, 0)

    def cross(g):
        remote_wait(prec_v.at[g, pl.ds(0, chips - 1)], precv.at[g, 1])
        for r in range(1, chips):
            ysend_v[g, r] = (pown_v[g, r] + prec_v[g, r].astype(F32)).astype(BF16)
            pltpu.make_async_remote_copy(
                src_ref=ysend_v.at[g, r], dst_ref=yrec_v.at[g, r],
                send_sem=ysend, recv_sem=yrecv.at[g],
                device_id={"tp": (y + r) % chips * 2 + 1 - core}, device_id_type=MESH,
            ).start()
        pown_v[g, 0] = down(g, 0)

    def leave(g):
        remote_wait(prec_v.at[g, 0], precv.at[g, 0])
        total = pown_v[g, 0] + prec_v[g, 0].astype(F32)
        remote_wait(yrec_v.at[g, pl.ds(0, chips - 1)], yrecv.at[g])
        for r in range(1, chips):
            total = total + yrec_v[g, r].astype(F32)
        weighted = (total * affc_v[g]).astype(BF16)
        folded = jnp.concatenate([weighted[:, h * fw:(h + 1) * fw] for h in range(fold)], axis=0)
        out = jnp.dot(spread_v[g], folded, preferred_element_type=F32)
        leave_v[g] = out.astype(BF16).reshape(experts, mr, fw)
        exchange(g, leave_v, ret_v, rsend, rrecv)

    def settle(g):
        remote_wait(ret_v.at[g], rrecv.at[g])
        update = jnp.dot(place_v[g], ret_v[g].reshape(rows, fw), preferred_element_type=F32)
        if g == 0:
            for h in range(fold):
                at = pl.ds(pl.multiple_of(col * share + h * fw, 128), fw)
                merged_v[h * tok:(h + 1) * tok, :] = x_v[:, at].astype(F32) + update[h * tok:(h + 1) * tok, :]
        else:
            merged_v[...] = merged_v[...] + update

    stages = {
        "s1": gather_start, "s2": gather_forward, "a": near, "m": middle, "b": away, "h": home,
        "x": cross, "l": leave, "r": settle,
    }
    if groups == 4:
        order = ORDER4
    else:
        order = [f"{name}.{g}" for name in ("s1", "s2", "a", "m", "b", "h", "x", "l", "r") for g in range(groups)]
    for item in order:
        name, g = item.split(".")
        with jax.named_scope(name + g):
            stages[name](int(g))

    square = 128
    eye = (
        lax.broadcasted_iota(I32, (square, square), 0)
        == lax.broadcasted_iota(I32, (square, square), 1)
    )
    merged = merged_v[...]
    both = jnp.sum(merged * merged, axis=1, keepdims=True)
    squares = both[0:tok]
    for h in range(1, fold):
        squares = squares + both[h * tok:(h + 1) * tok]
    for b in range(tok // square):
        line = jnp.sum(
            jnp.where(eye, squares[b * square:(b + 1) * square, :], 0.0), axis=0, keepdims=True
        )
        ssq_v[0, :, b * square:(b + 1) * square] = jnp.broadcast_to(line, (8, square))

    def square_copy(r):
        return pltpu.make_async_remote_copy(
            src_ref=ssq_v.at[0], dst_ref=ssq_v.at[r],
            send_sem=qsend, recv_sem=qrecv,
            device_id={"tp": (col + r) % tp}, device_id_type=MESH,
        )

    for r in range(1, tp):
        square_copy(r).start()
    small[3].wait()
    closing = fgain_v[...].astype(F32)
    fgain = jnp.concatenate([closing[i:i + 1, :] for i in range(lines)], axis=1)
    sums = ssq_v[0]
    with jax.named_scope("sqw"):
        remote_wait(ssq_v.at[pl.ds(1, tp - 1)], qrecv)
        for r in range(1, tp):
            sums = sums + ssq_v[r]
    scales = lax.rsqrt(sums[0:1, :] / width + EPSILON)
    for b in range(tok // square):
        line = scales[:, b * square:(b + 1) * square]
        column = jnp.sum(jnp.where(eye, line, 0.0), axis=1, keepdims=True)
        for h in range(fold):
            part = merged_v[h * tok + b * square:h * tok + (b + 1) * square, :]
            out_ref[b * square:(b + 1) * square, h * fw:(h + 1) * fw] = (
                part * column * fgain[:, h * fw:(h + 1) * fw]
            ).astype(BF16)

    with jax.named_scope("fin"):
        remote_wait(send_v, dsend)
        if full:
            remote_wait(sendf_v, hsend)
        remote_wait(piece_v.at[pl.ds(0, groups - full), pl.ds(0, chips - 1)], gsend)
        remote_wait(piece_v.at[:, pl.ds(0, chips)], fsend)
        remote_wait(psend_v, psend)
        remote_wait(ysend_v.at[:, pl.ds(0, chips - 1)], ysend)
        remote_wait(leave_v, rsend)
        remote_wait(ssq_v.at[pl.ds(1, tp - 1)], qsend)


ORDER4 = [
    "s1.0", "a.0", "s1.1", "s2.0", "m.0", "a.1", "b.0", "s1.2", "h.0", "s2.1", "x.0", "m.1",
    "a.2", "b.1", "h.1", "s2.2", "x.1", "m.2", "b.2", "l.0", "s1.3", "h.2", "a.3", "x.2",
    "l.1", "b.3", "h.3", "x.3", "l.2", "r.0", "l.3", "r.1", "r.2", "r.3",
]


def on_device(stream, ffn_gain, chosen, affinity, w_gate, w_up, w_down, final_gain):
    tok, width = stream.shape
    experts, caps = chosen.shape
    tp = lax.axis_size("tp")
    share = width // tp
    hid = w_gate.shape[2]
    slots = 3 * tok // 16
    groups, fold = (4, 2) if share % 256 == 0 else (2, 1)
    fw = share // fold
    cg = caps // groups
    mr = slots // groups * fold
    rows = experts * mr
    chips = tp // 2
    full = int(groups == 4 and chips == 2)
    hbm = pl.BlockSpec(memory_space=pltpu.HBM)
    dma = pltpu.SemaphoreType.DMA
    buffers = [
        pltpu.VMEM((tok, width), BF16),
        pltpu.VMEM((fold * tok, fw), BF16),
        pltpu.VMEM((fold * tok, fw) if full else (8, 128), BF16),
        pltpu.VMEM((tok, 1) if full else (8, 128), F32),
        pltpu.VMEM((width // 128, 128), BF16),
        pltpu.VMEM((width // 128, 128), F32),
        pltpu.VMEM((experts, caps), I32),
        pltpu.VMEM((1, caps), F32),
        pltpu.VMEM((share // 128, 128), BF16),
        pltpu.VMEM((width, hid), BF16),
        pltpu.VMEM((width, hid), BF16),
        pltpu.VMEM((tp, hid, share), BF16),
        pltpu.VMEM((groups, experts, mr, fold * tok), BF16),
        pltpu.VMEM((groups, fold * tok, rows), BF16),
        pltpu.VMEM((groups, fold * cg, rows), BF16),
        pltpu.VMEM((groups, rows, fold * cg), BF16),
        pltpu.VMEM((groups, cg, 1), F32),
        pltpu.VMEM((groups, experts, mr, fw), BF16),
        pltpu.VMEM((groups, experts, mr, fw), BF16),
        pltpu.VMEM((experts, mr, fw), BF16),
        pltpu.VMEM((experts, mr, fw), BF16),
        pltpu.VMEM((groups, tp, fold * cg, fw), BF16),
        pltpu.VMEM((groups, cg, hid), F32),
        pltpu.VMEM((groups, cg, hid), F32),
        pltpu.VMEM((groups, cg, hid), BF16),
        pltpu.VMEM((groups, chips, cg, share), BF16),
        pltpu.VMEM((groups, chips, cg, share), F32),
        pltpu.VMEM((groups, chips, cg, share), BF16),
        pltpu.VMEM((groups, chips, cg, share), BF16),
        pltpu.VMEM((groups, chips, cg, share), BF16),
        pltpu.VMEM((groups, experts, mr, fw), BF16),
        pltpu.VMEM((groups, experts, mr, fw), BF16),
        pltpu.VMEM((fold * tok, fw), F32),
        pltpu.VMEM((tp, 8, tok), F32),
    ]
    return pl.pallas_call(
        functools.partial(layer, experts, tp, groups, fold, slots, full),
        out_shape=pltpu.VMEM((tok, share), BF16),
        in_specs=[hbm] * 8,
        out_specs=pl.BlockSpec(memory_space=pltpu.VMEM),
        scratch_shapes=buffers + [
            dma((2,)), dma((4,)), dma((3,)), dma((3,)), dma,
            dma, dma((groups,)), dma, dma((groups,)), dma, dma((groups, 2)),
            dma, dma((groups, 2)), dma, dma((groups,)), dma, dma((groups,)), dma, dma, dma, dma,
        ],
        compiler_params=pltpu.CompilerParams(
            collective_id=0, has_side_effects=True, vmem_limit_bytes=56 * 1024 * 1024
        ),
        name="layer",
    )(
        stream,
        ffn_gain.reshape(width // 128, 128),
        chosen,
        affinity,
        w_gate[0],
        w_up[0],
        w_down[0],
        final_gain.reshape(share // 128, 128),
    )


def solution(mesh):
    return jax.shard_map(
        on_device,
        mesh=mesh,
        in_specs=(
            P("ep", None),
            P(),
            P(),
            P("ep", None),
            P("ep", None, "tp"),
            P("ep", None, "tp"),
            P("ep", "tp", None),
            P("tp"),
        ),
        out_specs=P("ep", "tp"),
        check_vma=False,
    )
```

```python
import functools

import jax
import jax.numpy as jnp
from jax import lax
from jax.experimental import pallas as pl
from jax.experimental.pallas import tpu as pltpu
from jax.sharding import PartitionSpec as P

EPSILON = 1e-06
F32 = jnp.float32
BF16 = jnp.bfloat16
I32 = jnp.int32
MESH = pl.DeviceIdType.MESH


def layer(
    experts, tp, groups, fold, slots, full,
    stream_hbm, gain_hbm, chosen_hbm, aff_hbm, wg_hbm, wu_hbm, wd_hbm, fgain_hbm,
    out_ref,
    x_v, xn_v, xf_v, scale_v, gain_v, gainf_v, chosen_v, aff_v, fgain_v, wg_v, wu_v, wd_v,
    sel_v, place_v, pack_v, spread_v, affc_v,
    send_v, recv_v, sendf_v, recvf_v, piece_v, accg_v, accu_v, hidden_v,
    psend_v, pown_v, prec_v, ysend_v, yrec_v, leave_v, ret_v, merged_v, ssq_v,
    x_sem, s_sem, wg_sem, wu_sem, wd_sem,
    dsend, drecv, gsend, grecv, fsend, frecv, psend, precv, ysend, yrecv,
    rsend, rrecv, qsend, qrecv, hsend, hrecv,
):
    me = lax.axis_index("ep")
    col = lax.axis_index("tp")
    tok, width = x_v.shape
    share = width // tp
    fw = share // fold
    caps = chosen_v.shape[1]
    cg = caps // groups
    sg = slots // groups
    mr = sg * fold
    rows = experts * mr
    chips = tp // 2
    y = col // 2
    core = col % 2
    partner = y * 2 + 1 - core

    barrier = pltpu.get_barrier_semaphore()
    for r in range(1, experts):
        pl.semaphore_signal(barrier, inc=1, device_id={"ep": (me + r) % experts, "tp": partner}, device_id_type=MESH)
    for r in range(1, tp):
        pl.semaphore_signal(barrier, inc=1, device_id={"tp": (col + r) % tp}, device_id_type=MESH)

    gather_cols = [col, partner]
    scatter_cols = [partner, col]
    for r in range(1, chips):
        before = (y + chips - r) % chips * 2
        after = (y + r) % chips * 2
        gather_cols += [before + 1 - core, before + core]
        scatter_cols += [after + core, after + 1 - core]

    small = []
    for n, (src, dst) in enumerate(
        ((chosen_hbm, chosen_v), (gain_hbm, gain_v), (aff_hbm, aff_v), (fgain_hbm, fgain_v))
    ):
        copy = pltpu.make_async_copy(src, dst, s_sem.at[n])
        copy.start()
        small.append(copy)
    pieces = x_sem.shape[0]
    xrows = tok // pieces
    x_copies = []
    for i in range(pieces):
        at = pl.ds(i * xrows, xrows)
        copy = pltpu.make_async_copy(stream_hbm.at[at, :], x_v.at[at, :], x_sem.at[i])
        copy.start()
        x_copies.append(copy)

    small[0].wait()
    base = (me * tok).astype(F32)
    lane_cap = lax.broadcasted_iota(I32, (mr, caps), 1)
    lane_tok = lax.broadcasted_iota(I32, (mr, tok), 1).astype(F32)
    sub = lax.broadcasted_iota(I32, (mr, 1), 0)
    sub_half = sum((jnp.where(sub >= h * sg, 1, 0) for h in range(1, fold)), jnp.zeros((mr, 1), I32))
    sub_slot = sub - sg * sub_half

    def build_sel(g):
        def one_expert(e, carry):
            row = chosen_v[pl.ds(e, 1), :].astype(F32)
            start = jnp.sum(jnp.where(row < base, 1.0, 0.0), axis=1, keepdims=True).astype(I32)
            first = start + ((g - start) & (groups - 1))
            hit = lane_cap == first + groups * sub_slot
            token = jnp.sum(jnp.where(hit, row + 1.0, 0.0), axis=1, keepdims=True) - 1.0 - base
            for h in range(fold):
                one = (token == lane_tok) & (sub_half == h)
                sel_v[g, e, :, h * tok:(h + 1) * tok] = jnp.where(one, 1.0, 0.0).astype(BF16)
            return carry

        lax.fori_loop(0, experts, one_expert, 0, unroll=experts <= 8)

    build_sel(0)
    small[1].wait()
    gainf_v[...] = gain_v[...].astype(F32)
    lines = share // 128

    def gain_of(which):
        return jnp.concatenate(
            [gainf_v[pl.ds(which * lines + i, 1), :] for i in range(lines)], axis=1
        )

    opposite = (y + 1) % chips * 2 + 1 - core
    gain = gain_of(partner)
    step = 32
    for i in range(pieces):
        x_copies[i].wait()
        if i == pieces - 1:
            for s, frm in enumerate(gather_cols):
                for src, dst, sem in ((wg_hbm, wg_v, wg_sem), (wu_hbm, wu_v, wu_sem)):
                    pltpu.make_async_copy(
                        src.at[pl.ds(frm * share, share), :],
                        dst.at[pl.ds(s * share, share), :],
                        sem,
                    ).start()
            for s, to in enumerate(scatter_cols):
                pltpu.make_async_copy(
                    wd_hbm.at[:, pl.ds(pl.multiple_of(to * share, 128), share)],
                    wd_v.at[s], wd_sem,
                ).start()
        for b in range(xrows // step):
            at = pl.ds(i * xrows + b * step, step)
            block = x_v[at, :].astype(F32)
            scale = lax.rsqrt(jnp.sum(block * block, axis=1, keepdims=True) / width + EPSILON)
            if full:
                scale_v[at, :] = scale
            own = x_v[at, pl.ds(pl.multiple_of(partner * share, 128), share)].astype(F32)
            normed = (own * scale * gain).astype(BF16)
            for h in range(fold):
                xn_v[pl.ds(h * tok + i * xrows + b * step, step), :] = normed[:, h * fw:(h + 1) * fw]

    far_first = sorted(range(experts), key=lambda r: -min(r, experts - r))
    def exchange(src, dst, ssem, rsem):
        for r in far_first:
            to = (me + r) % experts
            pltpu.make_async_remote_copy(
                src_ref=src.at[to], dst_ref=dst.at[me],
                send_sem=ssem, recv_sem=rsem,
                device_id={"ep": to, "tp": partner}, device_id_type=MESH,
            ).start()

    def dispatch(g):
        exchange(send_v.at[g], recv_v.at[g], dsend, drecv.at[g])

    def dispatch_more(g):
        exchange(sendf_v, recvf_v, hsend, hrecv)

    def remote_wait(ref, sem):
        pltpu.make_async_copy(ref, ref, sem).wait()

    window = 2
    for g in range(groups):
        if g > 0:
            build_sel(g)
        out = jnp.dot(sel_v[g].reshape(rows, fold * tok), xn_v[...], preferred_element_type=F32)
        send_v[g] = out.astype(BF16).reshape(experts, mr, fw)
        if full and g == groups - 1:
            gain_more = gain_of(opposite)
            for b in range(tok // step):
                at = pl.ds(b * step, step)
                own = x_v[at, pl.ds(pl.multiple_of(opposite * share, 128), share)].astype(F32)
                normed = (own * scale_v[at, :] * gain_more).astype(BF16)
                for h in range(fold):
                    xf_v[pl.ds(h * tok + b * step, step), :] = normed[:, h * fw:(h + 1) * fw]
            out = jnp.dot(sel_v[g].reshape(rows, fold * tok), xf_v[...], preferred_element_type=F32)
            sendf_v[...] = out.astype(BF16).reshape(experts, mr, fw)
        if g == 0:
            pl.semaphore_wait(barrier, experts - 1 + tp - 1)
        if g < window:
            dispatch(g)

    own_row = chosen_v[pl.ds(me, 1), :].astype(F32)

    def positions(axis):
        shape = (rows, 1) if axis == 0 else (1, rows)
        j = lax.broadcasted_iota(I32, shape, axis)
        start = jnp.zeros(shape, F32)
        end = jnp.zeros(shape, F32)
        within = j
        cut = jnp.zeros((1, 1), F32)
        for d in range(experts):
            mine = (j >= d * mr) & (j < (d + 1) * mr)
            after = jnp.sum(jnp.where(own_row < float((d + 1) * tok), 1.0, 0.0), axis=1, keepdims=True)
            start = start + jnp.where(mine, cut, 0.0)
            end = end + jnp.where(mine, after, 0.0)
            within = within - jnp.where(mine, d * mr, 0)
            cut = after
        half = sum((jnp.where(within >= h * sg, 1, 0) for h in range(1, fold)), jnp.zeros(shape, I32))
        return start.astype(I32), end.astype(I32), half, within - sg * half

    for axis, dst in ((1, pack_v), (0, spread_v)):
        start, end, half, slot = positions(axis)
        for g in range(groups):
            want = start + ((g - start) & (groups - 1)) + groups * slot
            want = jnp.where(want < end, want, -1)
            for h in range(fold):
                aim = jnp.where(half == h, want, -1)
                if axis == 1:
                    pick = lax.broadcasted_iota(I32, (cg, rows), 0) * groups + g
                    pack_v[g, h * cg:(h + 1) * cg, :] = jnp.where(pick == aim, 1.0, 0.0).astype(BF16)
                else:
                    pick = lax.broadcasted_iota(I32, (rows, cg), 1) * groups + g
                    spread_v[g, :, h * cg:(h + 1) * cg] = jnp.where(pick == aim, 1.0, 0.0).astype(BF16)

    small[2].wait()
    for g in range(groups):
        lane = lax.broadcasted_iota(I32, (cg, caps), 1)
        pick = lax.broadcasted_iota(I32, (cg, caps), 0) * groups + g
        affc_v[g] = jnp.sum(jnp.where(lane == pick, aff_v[...], 0.0), axis=1, keepdims=True)

    for g in range(groups):
        whole = sel_v[g].reshape(rows, fold * tok).astype(F32)
        place_v[g] = whole.T.astype(BF16)

    def gather_start(g):
        remote_wait(recv_v.at[g], drecv.at[g])
        if window <= g + window < groups - full:
            dispatch(g + window)
        got = recv_v[g].reshape(rows, fw)
        piece_v[g, 0] = jnp.dot(pack_v[g], got, preferred_element_type=F32).astype(BF16)
        if full and g == groups - 1:
            forward(g, 0)
            remote_wait(recvf_v, hrecv)
            got = recvf_v[...].reshape(rows, fw)
            piece_v[g, 3] = jnp.dot(pack_v[g], got, preferred_element_type=F32).astype(BF16)
            pltpu.make_async_remote_copy(
                src_ref=piece_v.at[g, 3], dst_ref=piece_v.at[g, 2],
                send_sem=fsend, recv_sem=frecv.at[g, 1],
                device_id={"tp": partner}, device_id_type=MESH,
            ).start()
            return
        for r in range(1, chips):
            pltpu.make_async_remote_copy(
                src_ref=piece_v.at[g, 0], dst_ref=piece_v.at[g, 2 * r],
                send_sem=gsend, recv_sem=grecv.at[g],
                device_id={"tp": (y + r) % chips * 2 + 1 - core}, device_id_type=MESH,
            ).start()
        forward(g, 0)

    def forward(g, r):
        pltpu.make_async_remote_copy(
            src_ref=piece_v.at[g, 2 * r], dst_ref=piece_v.at[g, 2 * r + 1],
            send_sem=fsend, recv_sem=frecv.at[g, min(r, 1)],
            device_id={"tp": partner}, device_id_type=MESH,
        ).start()

    def gather_forward(g):
        remote_wait(piece_v.at[g, pl.ds(0, chips - 1)], grecv.at[g])
        for r in range(1, chips):
            forward(g, r)

    waited = set()

    def weight_wait(n):
        if n not in waited:
            waited.add(n)
            remote_wait((wg_v, wu_v, wd_v)[n], (wg_sem, wu_sem, wd_sem)[n])

    def contract(g, slots_in):
        taken = jnp.concatenate(
            [piece_v[g, s, h * cg:(h + 1) * cg, :] for s in slots_in for h in range(fold)], axis=1
        )
        if slots_in == [0, 1]:
            return [
                jnp.dot(taken, w[0:2 * share, :], preferred_element_type=F32) for w in (wg_v, wu_v)
            ]
        return [
            sum(
                jnp.dot(
                    taken[:, n * share:(n + 1) * share], w[s * share:(s + 1) * share, :],
                    preferred_element_type=F32,
                )
                for n, s in enumerate(slots_in)
            )
            for w in (wg_v, wu_v)
        ]

    def near(g):
        weight_wait(0)
        weight_wait(1)
        if full and g == groups - 1:
            accg_v[g], accu_v[g] = contract(g, [0, 3])
            return
        remote_wait(piece_v.at[g, 1], frecv.at[g, 0])
        accg_v[g], accu_v[g] = contract(g, [0, 1])

    def middle(g):
        gate, up = contract(g, [2 * r for r in range(1, chips)])
        accg_v[g] += gate
        accu_v[g] += up

    def away(g):
        remote_wait(piece_v.at[g, pl.ds(0, chips - 1)], frecv.at[g, 1])
        if full and g == groups - 1:
            remote_wait(piece_v.at[g, 1], frecv.at[g, 0])
            gate, up = contract(g, [1, 2])
        else:
            gate, up = contract(g, [2 * r + 1 for r in range(1, chips)])
        gate = gate + accg_v[g]
        up = up + accu_v[g]
        hidden_v[g] = (gate / (1.0 + jnp.exp(-gate)) * up).astype(BF16)
        weight_wait(2)
        for r in range(1, chips):
            pair(g, r)

    def down(g, s):
        return jnp.dot(hidden_v[g], wd_v[s], preferred_element_type=F32)

    def pair(g, r):
        psend_v[g, r] = down(g, 2 * r + 1).astype(BF16)
        pltpu.make_async_remote_copy(
            src_ref=psend_v.at[g, r], dst_ref=prec_v.at[g, r],
            send_sem=psend, recv_sem=precv.at[g, min(r, 1)],
            device_id={"tp": partner}, device_id_type=MESH,
        ).start()

    def home(g):
        for r in range(1, chips):
            pown_v[g, r] = down(g, 2 * r)
        pair(g, 0)

    def cross(g):
        remote_wait(prec_v.at[g, pl.ds(0, chips - 1)], precv.at[g, 1])
        for r in range(1, chips):
            ysend_v[g, r] = (pown_v[g, r] + prec_v[g, r].astype(F32)).astype(BF16)
            pltpu.make_async_remote_copy(
                src_ref=ysend_v.at[g, r], dst_ref=yrec_v.at[g, r],
                send_sem=ysend, recv_sem=yrecv.at[g],
                device_id={"tp": (y + r) % chips * 2 + 1 - core}, device_id_type=MESH,
            ).start()
        pown_v[g, 0] = down(g, 0)

    def leave(g):
        remote_wait(prec_v.at[g, 0], precv.at[g, 0])
        total = pown_v[g, 0] + prec_v[g, 0].astype(F32)
        remote_wait(yrec_v.at[g, pl.ds(0, chips - 1)], yrecv.at[g])
        for r in range(1, chips):
            total = total + yrec_v[g, r].astype(F32)
        weighted = (total * affc_v[g]).astype(BF16)
        folded = jnp.concatenate([weighted[:, h * fw:(h + 1) * fw] for h in range(fold)], axis=0)
        out = jnp.dot(spread_v[g], folded, preferred_element_type=F32)
        leave_v[g] = out.astype(BF16).reshape(experts, mr, fw)
        exchange(leave_v.at[g], ret_v.at[g], rsend, rrecv.at[g])

    def settle(g):
        remote_wait(ret_v.at[g], rrecv.at[g])
        update = jnp.dot(place_v[g], ret_v[g].reshape(rows, fw), preferred_element_type=F32)
        if g == 0:
            for h in range(fold):
                at = pl.ds(pl.multiple_of(col * share + h * fw, 128), fw)
                merged_v[h * tok:(h + 1) * tok, :] = x_v[:, at].astype(F32) + update[h * tok:(h + 1) * tok, :]
        else:
            merged_v[...] = merged_v[...] + update

    stages = {
        "d": dispatch, "e": dispatch_more,
        "s1": gather_start, "s2": gather_forward, "a": near, "m": middle, "b": away, "h": home,
        "x": cross, "l": leave, "r": settle,
    }
    if groups == 4:
        order = ORDER4
    else:
        order = [f"{name}.{g}" for name in ("s1", "s2", "a", "m", "b", "h", "x", "l", "r") for g in range(groups)]
    for item in order:
        name, g = item.split(".")
        with jax.named_scope(name + g):
            stages[name](int(g))

    square = 128
    eye = (
        lax.broadcasted_iota(I32, (square, square), 0)
        == lax.broadcasted_iota(I32, (square, square), 1)
    )
    merged = merged_v[...]
    both = jnp.sum(merged * merged, axis=1, keepdims=True)
    squares = both[0:tok]
    for h in range(1, fold):
        squares = squares + both[h * tok:(h + 1) * tok]
    for b in range(tok // square):
        line = jnp.sum(
            jnp.where(eye, squares[b * square:(b + 1) * square, :], 0.0), axis=0, keepdims=True
        )
        ssq_v[0, :, b * square:(b + 1) * square] = line

    def square_copy(r):
        return pltpu.make_async_remote_copy(
            src_ref=ssq_v.at[0], dst_ref=ssq_v.at[r],
            send_sem=qsend, recv_sem=qrecv,
            device_id={"tp": (col + r) % tp}, device_id_type=MESH,
        )

    for r in range(1, tp):
        square_copy(r).start()
    small[3].wait()
    closing = fgain_v[...].astype(F32)
    fgain = jnp.concatenate([closing[i:i + 1, :] for i in range(lines)], axis=1)
    sums = ssq_v[0]
    with jax.named_scope("sqw"):
        remote_wait(ssq_v.at[pl.ds(1, tp - 1)], qrecv)
        for r in range(1, tp):
            sums = sums + ssq_v[r]
    scales = lax.rsqrt(sums[0:1, :] / width + EPSILON)
    for b in range(tok // square):
        line = scales[:, b * square:(b + 1) * square]
        column = jnp.sum(jnp.where(eye, line, 0.0), axis=1, keepdims=True)
        for h in range(fold):
            part = merged_v[h * tok + b * square:h * tok + (b + 1) * square, :]
            out_ref[b * square:(b + 1) * square, h * fw:(h + 1) * fw] = (
                part * column * fgain[:, h * fw:(h + 1) * fw]
            ).astype(BF16)

    with jax.named_scope("fin"):
        remote_wait(send_v, dsend)
        if full:
            remote_wait(sendf_v, hsend)
        remote_wait(piece_v.at[pl.ds(0, groups - full), pl.ds(0, chips - 1)], gsend)
        remote_wait(piece_v.at[:, pl.ds(0, chips)], fsend)
        remote_wait(psend_v, psend)
        remote_wait(ysend_v.at[:, pl.ds(0, chips - 1)], ysend)
        remote_wait(leave_v, rsend)
        remote_wait(ssq_v.at[pl.ds(1, tp - 1)], qsend)


ORDER4 = [
    "s1.0", "a.0", "s1.1", "d.3", "s2.0", "m.0", "a.1", "b.0", "e.3", "s1.2", "h.0", "s2.1",
    "x.0", "m.1", "a.2", "b.1", "h.1", "s2.2", "x.1", "m.2", "b.2", "l.0", "s1.3", "h.2",
    "a.3", "x.2", "l.1", "b.3", "h.3", "x.3", "l.2", "r.0", "l.3", "r.1", "r.2", "r.3",
]


def on_device(stream, ffn_gain, chosen, affinity, w_gate, w_up, w_down, final_gain):
    tok, width = stream.shape
    experts, caps = chosen.shape
    tp = lax.axis_size("tp")
    share = width // tp
    hid = w_gate.shape[2]
    slots = 3 * tok // 16
    groups, fold = (4, 2) if share % 256 == 0 else (2, 1)
    fw = share // fold
    cg = caps // groups
    mr = slots // groups * fold
    rows = experts * mr
    chips = tp // 2
    full = int(groups == 4 and chips == 2)
    hbm = pl.BlockSpec(memory_space=pltpu.HBM)
    dma = pltpu.SemaphoreType.DMA
    buffers = [
        pltpu.VMEM((tok, width), BF16),
        pltpu.VMEM((fold * tok, fw), BF16),
        pltpu.VMEM((fold * tok, fw) if full else (8, 128), BF16),
        pltpu.VMEM((tok, 1) if full else (8, 128), F32),
        pltpu.VMEM((width // 128, 128), BF16),
        pltpu.VMEM((width // 128, 128), F32),
        pltpu.VMEM((experts, caps), I32),
        pltpu.VMEM((1, caps), F32),
        pltpu.VMEM((share // 128, 128), BF16),
        pltpu.VMEM((width, hid), BF16),
        pltpu.VMEM((width, hid), BF16),
        pltpu.VMEM((tp, hid, share), BF16),
        pltpu.VMEM((groups, experts, mr, fold * tok), BF16),
        pltpu.VMEM((groups, fold * tok, rows), BF16),
        pltpu.VMEM((groups, fold * cg, rows), BF16),
        pltpu.VMEM((groups, rows, fold * cg), BF16),
        pltpu.VMEM((groups, cg, 1), F32),
        pltpu.VMEM((groups, experts, mr, fw), BF16),
        pltpu.VMEM((groups, experts, mr, fw), BF16),
        pltpu.VMEM((experts, mr, fw), BF16),
        pltpu.VMEM((experts, mr, fw), BF16),
        pltpu.VMEM((groups, tp, fold * cg, fw), BF16),
        pltpu.VMEM((groups, cg, hid), F32),
        pltpu.VMEM((groups, cg, hid), F32),
        pltpu.VMEM((groups, cg, hid), BF16),
        pltpu.VMEM((groups, chips, cg, share), BF16),
        pltpu.VMEM((groups, chips, cg, share), F32),
        pltpu.VMEM((groups, chips, cg, share), BF16),
        pltpu.VMEM((groups, chips, cg, share), BF16),
        pltpu.VMEM((groups, chips, cg, share), BF16),
        pltpu.VMEM((groups, experts, mr, fw), BF16),
        pltpu.VMEM((groups, experts, mr, fw), BF16),
        pltpu.VMEM((fold * tok, fw), F32),
        pltpu.VMEM((tp, 1, tok), F32),
    ]
    return pl.pallas_call(
        functools.partial(layer, experts, tp, groups, fold, slots, full),
        out_shape=pltpu.VMEM((tok, share), BF16),
        in_specs=[hbm] * 8,
        out_specs=pl.BlockSpec(memory_space=pltpu.VMEM),
        scratch_shapes=buffers + [
            dma((2,)), dma((4,)), dma, dma, dma,
            dma, dma((groups,)), dma, dma((groups,)), dma, dma((groups, 2)),
            dma, dma((groups, 2)), dma, dma((groups,)), dma, dma((groups,)), dma, dma, dma, dma,
        ],
        compiler_params=pltpu.CompilerParams(
            collective_id=0, has_side_effects=True, vmem_limit_bytes=56 * 1024 * 1024
        ),
        name="layer",
    )(
        stream,
        ffn_gain.reshape(width // 128, 128),
        chosen,
        affinity,
        w_gate[0],
        w_up[0],
        w_down[0],
        final_gain.reshape(share // 128, 128),
    )


def solution(mesh):
    return jax.shard_map(
        on_device,
        mesh=mesh,
        in_specs=(
            P("ep", None),
            P(),
            P(),
            P("ep", None),
            P("ep", None, "tp"),
            P("ep", None, "tp"),
            P("ep", "tp", None),
            P("tp"),
        ),
        out_specs=P("ep", "tp"),
        check_vma=False,
    )
```

```python
import functools

import jax
import jax.numpy as jnp
from jax import lax
from jax.experimental import pallas as pl
from jax.experimental.pallas import tpu as pltpu
from jax.sharding import PartitionSpec as P

EPSILON = 1e-06
F32 = jnp.float32
BF16 = jnp.bfloat16
I32 = jnp.int32
MESH = pl.DeviceIdType.MESH


def layer(
    experts, tp, groups, fold, slots, full,
    stream_hbm, gain_hbm, chosen_hbm, aff_hbm, wg_hbm, wu_hbm, wd_hbm, fgain_hbm,
    out_ref,
    x_v, xn_v, xf_v, scale_v, gain_v, gainf_v, chosen_v, aff_v, fgain_v, wg_v, wu_v, wd_v,
    sel_v, place_v, pack_v, spread_v, affc_v,
    send_v, recv_v, sendf_v, recvf_v, piece_v, accg_v, accu_v, hidden_v,
    psend_v, pown_v, prec_v, ysend_v, yrec_v, leave_v, ret_v, merged_v, ssq_v,
    x_sem, s_sem, wg_sem, wu_sem, wd_sem,
    dsend, drecv, gsend, grecv, fsend, frecv, psend, precv, ysend, yrecv,
    rsend, rrecv, qsend, qrecv, hsend, hrecv,
):
    me = lax.axis_index("ep")
    col = lax.axis_index("tp")
    tok, width = x_v.shape
    share = width // tp
    fw = share // fold
    caps = chosen_v.shape[1]
    cg = caps // groups
    sg = slots // groups
    mr = sg * fold
    rows = experts * mr
    chips = tp // 2
    y = col // 2
    core = col % 2
    partner = y * 2 + 1 - core

    barrier = pltpu.get_barrier_semaphore()
    for r in range(1, experts):
        pl.semaphore_signal(barrier, inc=1, device_id={"ep": (me + r) % experts, "tp": partner}, device_id_type=MESH)
    for r in range(1, tp):
        pl.semaphore_signal(barrier, inc=1, device_id={"tp": (col + r) % tp}, device_id_type=MESH)

    gather_cols = [col, partner]
    scatter_cols = [partner, col]
    for r in range(1, chips):
        before = (y + chips - r) % chips * 2
        after = (y + r) % chips * 2
        gather_cols += [before + 1 - core, before + core]
        scatter_cols += [after + core, after + 1 - core]

    small = []
    for n, (src, dst) in enumerate(
        ((chosen_hbm, chosen_v), (gain_hbm, gain_v), (aff_hbm, aff_v), (fgain_hbm, fgain_v))
    ):
        copy = pltpu.make_async_copy(src, dst, s_sem.at[n])
        copy.start()
        small.append(copy)
    pieces = x_sem.shape[0]
    xrows = tok // pieces
    x_copies = []
    for i in range(pieces):
        at = pl.ds(i * xrows, xrows)
        copy = pltpu.make_async_copy(stream_hbm.at[at, :], x_v.at[at, :], x_sem.at[i])
        copy.start()
        x_copies.append(copy)

    small[0].wait()
    base = (me * tok).astype(F32)
    lane_cap = lax.broadcasted_iota(I32, (mr, caps), 1)
    lane_tok = lax.broadcasted_iota(I32, (mr, tok), 1).astype(F32)
    sub = lax.broadcasted_iota(I32, (mr, 1), 0)
    sub_half = sum((jnp.where(sub >= h * sg, 1, 0) for h in range(1, fold)), jnp.zeros((mr, 1), I32))
    sub_slot = sub - sg * sub_half

    def build_sel(g):
        def one_expert(e, carry):
            row = chosen_v[pl.ds(e, 1), :].astype(F32)
            start = jnp.sum(jnp.where(row < base, 1.0, 0.0), axis=1, keepdims=True).astype(I32)
            first = start + ((g - start) & (groups - 1))
            hit = lane_cap == first + groups * sub_slot
            token = jnp.sum(jnp.where(hit, row + 1.0, 0.0), axis=1, keepdims=True) - 1.0 - base
            for h in range(fold):
                one = (token == lane_tok) & (sub_half == h)
                sel_v[g, e, :, h * tok:(h + 1) * tok] = jnp.where(one, 1.0, 0.0).astype(BF16)
            return carry

        lax.fori_loop(0, experts, one_expert, 0, unroll=experts <= 8)

    build_sel(0)
    small[1].wait()
    gainf_v[...] = gain_v[...].astype(F32)
    lines = share // 128

    def gain_of(which):
        return jnp.concatenate(
            [gainf_v[pl.ds(which * lines + i, 1), :] for i in range(lines)], axis=1
        )

    opposite = (y + 1) % chips * 2 + 1 - core
    gain = gain_of(partner)
    step = 32
    for i in range(pieces):
        x_copies[i].wait()
        if i == pieces - 1:
            for s, frm in enumerate(gather_cols):
                for src, dst, sem in ((wg_hbm, wg_v, wg_sem), (wu_hbm, wu_v, wu_sem)):
                    pltpu.make_async_copy(
                        src.at[pl.ds(frm * share, share), :],
                        dst.at[pl.ds(s * share, share), :],
                        sem,
                    ).start()
            for s, to in enumerate(scatter_cols):
                pltpu.make_async_copy(
                    wd_hbm.at[:, pl.ds(pl.multiple_of(to * share, 128), share)],
                    wd_v.at[s], wd_sem,
                ).start()
        for b in range(xrows // step):
            at = pl.ds(i * xrows + b * step, step)
            block = x_v[at, :].astype(F32)
            scale = lax.rsqrt(jnp.sum(block * block, axis=1, keepdims=True) / width + EPSILON)
            if full:
                scale_v[at, :] = scale
            own = x_v[at, pl.ds(pl.multiple_of(partner * share, 128), share)].astype(F32)
            normed = (own * scale * gain).astype(BF16)
            for h in range(fold):
                xn_v[pl.ds(h * tok + i * xrows + b * step, step), :] = normed[:, h * fw:(h + 1) * fw]

    far_first = sorted(range(experts), key=lambda r: -min(r, experts - r))
    def exchange(src, dst, ssem, rsem):
        for r in far_first:
            to = (me + r) % experts
            pltpu.make_async_remote_copy(
                src_ref=src.at[to], dst_ref=dst.at[me],
                send_sem=ssem, recv_sem=rsem,
                device_id={"ep": to, "tp": partner}, device_id_type=MESH,
            ).start()

    def dispatch(g):
        exchange(send_v.at[g], recv_v.at[g], dsend, drecv.at[g])

    def dispatch_more(g):
        exchange(sendf_v, recvf_v, hsend, hrecv)

    def remote_wait(ref, sem):
        pltpu.make_async_copy(ref, ref, sem).wait()

    window = 2
    for g in range(groups):
        if g > 0:
            build_sel(g)
        out = jnp.dot(sel_v[g].reshape(rows, fold * tok), xn_v[...], preferred_element_type=F32)
        send_v[g] = out.astype(BF16).reshape(experts, mr, fw)
        if full and g == groups - 1:
            gain_more = gain_of(opposite)
            for b in range(tok // step):
                at = pl.ds(b * step, step)
                own = x_v[at, pl.ds(pl.multiple_of(opposite * share, 128), share)].astype(F32)
                normed = (own * scale_v[at, :] * gain_more).astype(BF16)
                for h in range(fold):
                    xf_v[pl.ds(h * tok + b * step, step), :] = normed[:, h * fw:(h + 1) * fw]
            out = jnp.dot(sel_v[g].reshape(rows, fold * tok), xf_v[...], preferred_element_type=F32)
            sendf_v[...] = out.astype(BF16).reshape(experts, mr, fw)
        if g == 0:
            pl.semaphore_wait(barrier, experts - 1 + tp - 1)
        if g < window:
            dispatch(g)

    own_row = chosen_v[pl.ds(me, 1), :].astype(F32)

    def positions(axis):
        shape = (rows, 1) if axis == 0 else (1, rows)
        j = lax.broadcasted_iota(I32, shape, axis)
        start = jnp.zeros(shape, F32)
        end = jnp.zeros(shape, F32)
        within = j
        cut = jnp.zeros((1, 1), F32)
        for d in range(experts):
            mine = (j >= d * mr) & (j < (d + 1) * mr)
            after = jnp.sum(jnp.where(own_row < float((d + 1) * tok), 1.0, 0.0), axis=1, keepdims=True)
            start = start + jnp.where(mine, cut, 0.0)
            end = end + jnp.where(mine, after, 0.0)
            within = within - jnp.where(mine, d * mr, 0)
            cut = after
        half = sum((jnp.where(within >= h * sg, 1, 0) for h in range(1, fold)), jnp.zeros(shape, I32))
        return start.astype(I32), end.astype(I32), half, within - sg * half

    for axis, dst in ((1, pack_v), (0, spread_v)):
        start, end, half, slot = positions(axis)
        for g in range(groups):
            want = start + ((g - start) & (groups - 1)) + groups * slot
            want = jnp.where(want < end, want, -1)
            for h in range(fold):
                aim = jnp.where(half == h, want, -1)
                if axis == 1:
                    pick = lax.broadcasted_iota(I32, (cg, rows), 0) * groups + g
                    pack_v[g, h * cg:(h + 1) * cg, :] = jnp.where(pick == aim, 1.0, 0.0).astype(BF16)
                else:
                    pick = lax.broadcasted_iota(I32, (rows, cg), 1) * groups + g
                    spread_v[g, :, h * cg:(h + 1) * cg] = jnp.where(pick == aim, 1.0, 0.0).astype(BF16)

    small[2].wait()
    for g in range(groups):
        lane = lax.broadcasted_iota(I32, (cg, caps), 1)
        pick = lax.broadcasted_iota(I32, (cg, caps), 0) * groups + g
        affc_v[g] = jnp.sum(jnp.where(lane == pick, aff_v[...], 0.0), axis=1, keepdims=True)

    for g in range(groups):
        whole = sel_v[g].reshape(rows, fold * tok).astype(F32)
        place_v[g] = whole.T.astype(BF16)

    def gather_start(g):
        remote_wait(recv_v.at[g], drecv.at[g])
        if window <= g + window < groups - full:
            dispatch(g + window)
        got = recv_v[g].reshape(rows, fw)
        piece_v[g, 0] = jnp.dot(pack_v[g], got, preferred_element_type=F32).astype(BF16)
        if full and g == groups - 1:
            forward(g, 0)
            remote_wait(recvf_v, hrecv)
            got = recvf_v[...].reshape(rows, fw)
            piece_v[g, 3] = jnp.dot(pack_v[g], got, preferred_element_type=F32).astype(BF16)
            pltpu.make_async_remote_copy(
                src_ref=piece_v.at[g, 3], dst_ref=piece_v.at[g, 2],
                send_sem=fsend, recv_sem=frecv.at[g, 1],
                device_id={"tp": partner}, device_id_type=MESH,
            ).start()
            return
        for r in range(1, chips):
            pltpu.make_async_remote_copy(
                src_ref=piece_v.at[g, 0], dst_ref=piece_v.at[g, 2 * r],
                send_sem=gsend, recv_sem=grecv.at[g],
                device_id={"tp": (y + r) % chips * 2 + 1 - core}, device_id_type=MESH,
            ).start()
        forward(g, 0)

    def forward(g, r):
        pltpu.make_async_remote_copy(
            src_ref=piece_v.at[g, 2 * r], dst_ref=piece_v.at[g, 2 * r + 1],
            send_sem=fsend, recv_sem=frecv.at[g, min(r, 1)],
            device_id={"tp": partner}, device_id_type=MESH,
        ).start()

    def gather_forward(g):
        remote_wait(piece_v.at[g, pl.ds(0, chips - 1)], grecv.at[g])
        for r in range(1, chips):
            forward(g, r)

    waited = set()

    def weight_wait(n):
        if n not in waited:
            waited.add(n)
            remote_wait((wg_v, wu_v, wd_v)[n], (wg_sem, wu_sem, wd_sem)[n])

    def contract(g, slots_in):
        taken = jnp.concatenate(
            [piece_v[g, s, h * cg:(h + 1) * cg, :] for s in slots_in for h in range(fold)], axis=1
        )
        if slots_in == [0, 1]:
            return [
                jnp.dot(taken, w[0:2 * share, :], preferred_element_type=F32) for w in (wg_v, wu_v)
            ]
        return [
            sum(
                jnp.dot(
                    taken[:, n * share:(n + 1) * share], w[s * share:(s + 1) * share, :],
                    preferred_element_type=F32,
                )
                for n, s in enumerate(slots_in)
            )
            for w in (wg_v, wu_v)
        ]

    def near(g):
        weight_wait(0)
        weight_wait(1)
        if full and g == groups - 1:
            accg_v[g], accu_v[g] = contract(g, [0, 3])
            return
        remote_wait(piece_v.at[g, 1], frecv.at[g, 0])
        accg_v[g], accu_v[g] = contract(g, [0, 1])

    def middle(g):
        gate, up = contract(g, [2 * r for r in range(1, chips)])
        accg_v[g] += gate
        accu_v[g] += up

    def away(g):
        remote_wait(piece_v.at[g, pl.ds(0, chips - 1)], frecv.at[g, 1])
        if full and g == groups - 1:
            remote_wait(piece_v.at[g, 1], frecv.at[g, 0])
            gate, up = contract(g, [1, 2])
        else:
            gate, up = contract(g, [2 * r + 1 for r in range(1, chips)])
        gate = gate + accg_v[g]
        up = up + accu_v[g]
        hidden_v[g] = (gate / (1.0 + jnp.exp(-gate)) * up).astype(BF16)
        weight_wait(2)
        for r in range(1, chips):
            pair(g, r)

    def down(g, s):
        return jnp.dot(hidden_v[g], wd_v[s], preferred_element_type=F32)

    def pair(g, r):
        psend_v[g, r] = down(g, 2 * r + 1).astype(BF16)
        pltpu.make_async_remote_copy(
            src_ref=psend_v.at[g, r], dst_ref=prec_v.at[g, r],
            send_sem=psend, recv_sem=precv.at[g, min(r, 1)],
            device_id={"tp": partner}, device_id_type=MESH,
        ).start()

    def home(g):
        for r in range(1, chips):
            pown_v[g, r] = down(g, 2 * r)
        pair(g, 0)

    def cross(g):
        remote_wait(prec_v.at[g, pl.ds(0, chips - 1)], precv.at[g, 1])
        for r in range(1, chips):
            ysend_v[g, r] = (pown_v[g, r] + prec_v[g, r].astype(F32)).astype(BF16)
            pltpu.make_async_remote_copy(
                src_ref=ysend_v.at[g, r], dst_ref=yrec_v.at[g, r],
                send_sem=ysend, recv_sem=yrecv.at[g],
                device_id={"tp": (y + r) % chips * 2 + 1 - core}, device_id_type=MESH,
            ).start()
        pown_v[g, 0] = down(g, 0)

    def leave(g):
        remote_wait(prec_v.at[g, 0], precv.at[g, 0])
        total = pown_v[g, 0] + prec_v[g, 0].astype(F32)
        remote_wait(yrec_v.at[g, pl.ds(0, chips - 1)], yrecv.at[g])
        for r in range(1, chips):
            total = total + yrec_v[g, r].astype(F32)
        weighted = (total * affc_v[g]).astype(BF16)
        folded = jnp.concatenate([weighted[:, h * fw:(h + 1) * fw] for h in range(fold)], axis=0)
        out = jnp.dot(spread_v[g], folded, preferred_element_type=F32)
        leave_v[g] = out.astype(BF16).reshape(experts, mr, fw)
        exchange(leave_v.at[g], ret_v.at[g], rsend, rrecv.at[g])

    def settle(g):
        remote_wait(ret_v.at[g], rrecv.at[g])
        update = jnp.dot(place_v[g], ret_v[g].reshape(rows, fw), preferred_element_type=F32)
        if g == 0:
            for h in range(fold):
                at = pl.ds(pl.multiple_of(col * share + h * fw, 128), fw)
                merged_v[h * tok:(h + 1) * tok, :] = x_v[:, at].astype(F32) + update[h * tok:(h + 1) * tok, :]
        else:
            merged_v[...] = merged_v[...] + update

    stages = {
        "d": dispatch, "e": dispatch_more,
        "s1": gather_start, "s2": gather_forward, "a": near, "m": middle, "b": away, "h": home,
        "x": cross, "l": leave, "r": settle,
    }
    if groups == 4:
        order = ORDER4
    else:
        order = [f"{name}.{g}" for name in ("s1", "s2", "a", "m", "b", "h", "x", "l", "r") for g in range(groups)]
    for item in order:
        name, g = item.split(".")
        with jax.named_scope(name + g):
            stages[name](int(g))

    square = 128
    eye = (
        lax.broadcasted_iota(I32, (square, square), 0)
        == lax.broadcasted_iota(I32, (square, square), 1)
    )
    merged = merged_v[...]
    both = jnp.sum(merged * merged, axis=1, keepdims=True)
    squares = both[0:tok]
    for h in range(1, fold):
        squares = squares + both[h * tok:(h + 1) * tok]
    for b in range(tok // square):
        line = jnp.sum(
            jnp.where(eye, squares[b * square:(b + 1) * square, :], 0.0), axis=0, keepdims=True
        )
        ssq_v[0, :, b * square:(b + 1) * square] = line

    def square_copy(r):
        return pltpu.make_async_remote_copy(
            src_ref=ssq_v.at[0], dst_ref=ssq_v.at[r],
            send_sem=qsend, recv_sem=qrecv,
            device_id={"tp": (col + r) % tp}, device_id_type=MESH,
        )

    for r in range(1, tp):
        square_copy(r).start()
    small[3].wait()
    closing = fgain_v[...].astype(F32)
    fgain = jnp.concatenate([closing[i:i + 1, :] for i in range(lines)], axis=1)
    sums = ssq_v[0]
    with jax.named_scope("sqw"):
        remote_wait(ssq_v.at[pl.ds(1, tp - 1)], qrecv)
        for r in range(1, tp):
            sums = sums + ssq_v[r]
    scales = lax.rsqrt(sums[0:1, :] / width + EPSILON)
    for b in range(tok // square):
        line = scales[:, b * square:(b + 1) * square]
        column = jnp.sum(jnp.where(eye, line, 0.0), axis=1, keepdims=True)
        for h in range(fold):
            part = merged_v[h * tok + b * square:h * tok + (b + 1) * square, :]
            out_ref[b * square:(b + 1) * square, h * fw:(h + 1) * fw] = (
                part * column * fgain[:, h * fw:(h + 1) * fw]
            ).astype(BF16)

    with jax.named_scope("fin"):
        remote_wait(send_v, dsend)
        if full:
            remote_wait(sendf_v, hsend)
        remote_wait(piece_v.at[pl.ds(0, groups - full), pl.ds(0, chips - 1)], gsend)
        remote_wait(piece_v.at[:, pl.ds(0, chips)], fsend)
        remote_wait(psend_v, psend)
        remote_wait(ysend_v.at[:, pl.ds(0, chips - 1)], ysend)
        remote_wait(leave_v, rsend)
        remote_wait(ssq_v.at[pl.ds(1, tp - 1)], qsend)


ORDER4 = [
    "s1.0", "a.0", "s1.1", "d.3", "s2.0", "m.0", "a.1", "b.0", "e.3", "s1.2", "h.0", "s2.1",
    "x.0", "m.1", "a.2", "b.1", "h.1", "s2.2", "x.1", "m.2", "s1.3", "b.2", "l.0", "h.2",
    "a.3", "x.2", "b.3", "l.1", "h.3", "x.3", "l.2", "r.0", "l.3", "r.1", "r.2", "r.3",
]


def on_device(stream, ffn_gain, chosen, affinity, w_gate, w_up, w_down, final_gain):
    tok, width = stream.shape
    experts, caps = chosen.shape
    tp = lax.axis_size("tp")
    share = width // tp
    hid = w_gate.shape[2]
    slots = 3 * tok // 16
    groups, fold = (4, 2) if share % 256 == 0 else (2, 1)
    fw = share // fold
    cg = caps // groups
    mr = slots // groups * fold
    rows = experts * mr
    chips = tp // 2
    full = int(groups == 4 and chips == 2)
    hbm = pl.BlockSpec(memory_space=pltpu.HBM)
    dma = pltpu.SemaphoreType.DMA
    buffers = [
        pltpu.VMEM((tok, width), BF16),
        pltpu.VMEM((fold * tok, fw), BF16),
        pltpu.VMEM((fold * tok, fw) if full else (8, 128), BF16),
        pltpu.VMEM((tok, 1) if full else (8, 128), F32),
        pltpu.VMEM((width // 128, 128), BF16),
        pltpu.VMEM((width // 128, 128), F32),
        pltpu.VMEM((experts, caps), I32),
        pltpu.VMEM((1, caps), F32),
        pltpu.VMEM((share // 128, 128), BF16),
        pltpu.VMEM((width, hid), BF16),
        pltpu.VMEM((width, hid), BF16),
        pltpu.VMEM((tp, hid, share), BF16),
        pltpu.VMEM((groups, experts, mr, fold * tok), BF16),
        pltpu.VMEM((groups, fold * tok, rows), BF16),
        pltpu.VMEM((groups, fold * cg, rows), BF16),
        pltpu.VMEM((groups, rows, fold * cg), BF16),
        pltpu.VMEM((groups, cg, 1), F32),
        pltpu.VMEM((groups, experts, mr, fw), BF16),
        pltpu.VMEM((groups, experts, mr, fw), BF16),
        pltpu.VMEM((experts, mr, fw), BF16),
        pltpu.VMEM((experts, mr, fw), BF16),
        pltpu.VMEM((groups, tp, fold * cg, fw), BF16),
        pltpu.VMEM((groups, cg, hid), F32),
        pltpu.VMEM((groups, cg, hid), F32),
        pltpu.VMEM((groups, cg, hid), BF16),
        pltpu.VMEM((groups, chips, cg, share), BF16),
        pltpu.VMEM((groups, chips, cg, share), F32),
        pltpu.VMEM((groups, chips, cg, share), BF16),
        pltpu.VMEM((groups, chips, cg, share), BF16),
        pltpu.VMEM((groups, chips, cg, share), BF16),
        pltpu.VMEM((groups, experts, mr, fw), BF16),
        pltpu.VMEM((groups, experts, mr, fw), BF16),
        pltpu.VMEM((fold * tok, fw), F32),
        pltpu.VMEM((tp, 1, tok), F32),
    ]
    return pl.pallas_call(
        functools.partial(layer, experts, tp, groups, fold, slots, full),
        out_shape=pltpu.VMEM((tok, share), BF16),
        in_specs=[hbm] * 8,
        out_specs=pl.BlockSpec(memory_space=pltpu.VMEM),
        scratch_shapes=buffers + [
            dma((2,)), dma((4,)), dma, dma, dma,
            dma, dma((groups,)), dma, dma((groups,)), dma, dma((groups, 2)),
            dma, dma((groups, 2)), dma, dma((groups,)), dma, dma((groups,)), dma, dma, dma, dma,
        ],
        compiler_params=pltpu.CompilerParams(
            collective_id=0, has_side_effects=True, vmem_limit_bytes=56 * 1024 * 1024
        ),
        name="layer",
    )(
        stream,
        ffn_gain.reshape(width // 128, 128),
        chosen,
        affinity,
        w_gate[0],
        w_up[0],
        w_down[0],
        final_gain.reshape(share // 128, 128),
    )


def solution(mesh):
    return jax.shard_map(
        on_device,
        mesh=mesh,
        in_specs=(
            P("ep", None),
            P(),
            P(),
            P("ep", None),
            P("ep", None, "tp"),
            P("ep", None, "tp"),
            P("ep", "tp", None),
            P("tp"),
        ),
        out_specs=P("ep", "tp"),
        check_vma=False,
    )
```
